256 devices in a mesh: ep: 64 (over z, x, core), tp: 4 (over y).
Axes of the slice: x: 4, y: 4, z: 8, core: 2. Of those that a mesh axis runs over, the one named last changes fastest.
Arguments:
- tokens: bfloat16 [65536, 2048], P(('ep', 'tp')), may hold values from -6 to 6
- norm_gain: bfloat16 [2048], replicated, may hold values from 0.099609375 to 1.8984375
- expert_ids: int32 [65536, 2], P(('ep', 'tp')), may hold values from 0 to 63, all different within a row; in each aligned block of 256 rows (0 to 255, 256 to 511, ...) at most 16 rows name the same one
- group_weight: float32 [65536], P(('ep', 'tp')), may hold values from 0.25 to 1
- expert_logit: float32 [65536, 2], P(('ep', 'tp')), may hold values from -4 to 4
- w_gate: bfloat16 [64, 2048, 1024], P('ep', None, 'tp'), may hold values from -0.125 to 0.125
- w_up: bfloat16 [64, 2048, 1024], P('ep', None, 'tp'), may hold values from -0.125 to 0.125
- w_down: bfloat16 [64, 1024, 2048], P('ep', 'tp')
- final_gain: bfloat16 [2048], P('tp'), may hold values from 0.099609375 to 1.8984375
Outputs:
- normed_out: bfloat16 [65536, 2048], P('ep', 'tp')
The draws below stay inside these ranges and needn't reach their ends.
Inputs may be any that keep to these rules, and one draw needn't show every extreme that they name: `expert_ids`: the 2 experts of a token differ. Among the rows of one device (aligned blocks of 256 tokens) no expert is named more than 16 times, a bound that some block reaches.
All inputs are finite; a program needn't handle non-finite values.
Results may differ from the reference program's by a relative error of at most 0.0058.
Values may be sent and summed in bfloat16 or wider, within the bound.
A program may use at most 128 MiB of HBM per device.

```python
import math
import jax
import jax.numpy as jnp
import numpy as np
from jax import lax

D = 2048
FF = 1024
TOP = 2
TOK_DEV = 256
EXPERTS = 64
CAP = 16
TOKENS = 65536


def draw_w_down(key, part):
    first, second = jax.random.split(key)
    base = jax.random.normal(first, (EXPERTS, FF, D), jnp.float32)
    levels = jnp.array([0.4, 0.9, 1.5, 2.4], jnp.float32)
    shuffled = levels[jax.random.permutation(second, 4)]
    quarter = jnp.arange(D, dtype=jnp.int32) * 4 // D
    column_scale = shuffled[quarter]
    return (base * FF ** (-0.5) * column_scale[None, None, :]).astype(jnp.bfloat16)


def block_levels(stream_key, extent, shards, smallest, largest):
    loudness, own = 1.0, jax.random.fold_in(stream_key, 6)
    for position, blocks in shards:
        heights = jnp.exp(jax.random.uniform(jax.random.fold_in(own, position), (blocks,), jnp.float32, smallest / len(shards), largest / len(shards)))
        loudness = loudness * jnp.repeat(heights, extent[position] // blocks).reshape([-1 if axis == position else 1 for axis in range(len(extent))])
    return loudness


def shared_out(key, own, number, rows, number_of, top, limit, slope):
    ranking = jax.random.permutation(key, number_of)
    packed, common = shares(number_of, rows * top, limit, slope, True), shares(number_of, rows * top, limit, slope, False)
    places = jnp.arange(number_of)

    def named(tallies, rotation):
        used = int((tallies > 0).sum())
        fixed = max(1, used // 4)
        passed = fixed + (places - fixed + rotation * (used - fixed)) % max(1, number_of - fixed)
        return jnp.zeros((number_of,), jnp.int32).at[ranking[jnp.where(places < fixed, places, passed)]].set(jnp.asarray(tallies, jnp.int32))

    tallies = jnp.where(number % 4 == 0, named(packed, number // 4), named(common, number - number // 4 - 1))
    mixed = jax.random.permutation(jax.random.fold_in(own, 3), number_of)
    giver, sink = mixed[0:number_of // 2 * 2:2], mixed[1:number_of // 2 * 2:2]
    slack = jnp.minimum(tallies[giver] - 1, limit - tallies[sink]) // 2
    slack = jnp.where((giver == ranking[0]) | (sink == ranking[0]) | (tallies[sink] == 0), 0, jnp.maximum(slack, 0))
    passed = jax.random.randint(jax.random.fold_in(own, 4), (number_of // 2,), 0, 1 << 20) % (slack + 1)
    tallies = tallies.at[giver].add(-passed).at[sink].add(passed)
    labels = jnp.searchsorted(jnp.cumsum(tallies), jnp.arange(rows * top), side="right").astype(jnp.int32)
    grid = labels.reshape(top, rows).T
    grid = grid[jax.random.permutation(jax.random.fold_in(own, 1), rows)]
    rotation = jax.random.randint(jax.random.fold_in(own, 2), (rows, 1), 0, top)
    return jnp.take_along_axis(grid, (jnp.arange(top)[None, :] + rotation) % top, axis=1)


def shares(count, total, reach, slope, full):
    loads = [(1 << 20) // math.isqrt(standing ** slope) + 1 for standing in range(1, count + 1)]
    largest = reach if full else min(reach, max(-(-total // count), total * loads[0] // sum(loads)))
    least = 1 if total - largest >= count - 1 else 0
    holding, spare = [largest] + [least] * (count - 1), total - largest - least * (count - 1)
    while spare > 0:
        candidates = [i for i in range(1, count) if holding[i] < largest] or [i for i in range(1, count) if holding[i] < reach]
        mass, remaining = sum([loads[i] for i in candidates]), spare
        for i in candidates:
            more = min(reach - holding[i], max(1, remaining * loads[i] // mass), spare)
            holding[i] = holding[i] + more
            spare = spare - more
    return np.array(holding)


def noise(key, dims, deviation, most, cuts=(), held_as=jnp.bfloat16):
    values = jax.random.normal(key, dims, jnp.float32) * deviation
    if len(cuts) > 0:
        values = block_levels(key, dims, cuts, -0.22, 0.18) * values
    return jnp.clip(values, min=-most, max=most).astype(held_as)


def setup_inputs(seed: int = 0) -> dict:
    key_list = jax.random.split(jax.random.key(seed), 10)
    tokens = noise(key_list[0], (TOKENS, D), 1.0, 6.0, ((0, 256),))
    norm_gain = jnp.clip(1.0 + 0.18 * jax.random.normal(key_list[1], (D,), jnp.float32), 0.099609375, 1.8984375).astype(jnp.bfloat16)
    expert_ids_keys = jax.random.split(jax.random.fold_in(key_list[2], 1), TOKENS // TOK_DEV)
    expert_ids_turns = jax.random.permutation(jax.random.fold_in(key_list[2], 3), TOKENS // TOK_DEV)
    expert_ids = jax.vmap(lambda own, number: shared_out(jax.random.fold_in(key_list[2], 2), own, number, TOK_DEV, EXPERTS, TOP, CAP, 2))(expert_ids_keys, expert_ids_turns).reshape((TOKENS, TOP))
    group_weight = jnp.clip(0.25 + 0.75 * jax.random.uniform(key_list[3], (TOKENS,), jnp.float32) ** block_levels(key_list[3], (TOKENS,), ((0, 256),), -0.2, 0.2), 0.25, 1.0)
    expert_logit = noise(key_list[4], (TOKENS, TOP), 1.5, 4.0, ((0, 256),), jnp.float32)
    w_gate = noise(key_list[5], (EXPERTS, D, FF), D ** -0.5, 0.125, ((0, 64), (2, 4)))
    w_up = noise(key_list[6], (EXPERTS, D, FF), D ** -0.5, 0.125, ((0, 64), (2, 4)))
    w_down = draw_w_down(jax.random.fold_in(key_list[9], 71), 0)
    final_gain = jnp.clip(1.0 + 0.18 * jax.random.normal(key_list[8], (D,), jnp.float32), 0.099609375, 1.8984375).astype(jnp.bfloat16)
    return dict(tokens=tokens, norm_gain=norm_gain, expert_ids=expert_ids, group_weight=group_weight, expert_logit=expert_logit, w_gate=w_gate, w_up=w_up, w_down=w_down, final_gain=final_gain)


EPS = 1e-06

def normalize(values, gain):
    return values * lax.rsqrt(lax.optimization_barrier(jnp.mean(values * values, axis=-1, keepdims=True)) + EPS) * gain.astype(jnp.float32)

def reference(tokens, norm_gain, expert_ids, group_weight, expert_logit, w_gate, w_up, w_down, final_gain):
    block_len = 256
    tokens_f = tokens.astype(jnp.float32)
    normed_in = normalize(tokens_f, norm_gain).astype(jnp.bfloat16)
    total_tok, per_token = expert_ids.shape
    experts = w_gate.shape[0]
    assigned = total_tok * per_token
    flat_ids = expert_ids.reshape(assigned).astype(jnp.int32)
    sort_order = jnp.argsort(flat_ids, stable=True).astype(jnp.int32)
    sorted_ids = flat_ids[sort_order]
    counts = jnp.bincount(flat_ids, length=experts).astype(jnp.int32)
    starts = (jnp.cumsum(counts) - counts).astype(jnp.int32)
    padded = (counts + block_len - 1) // block_len * block_len
    ends = jnp.cumsum(padded).astype(jnp.int32)
    pad_starts = (ends - padded).astype(jnp.int32)
    target = (pad_starts[sorted_ids] + jnp.arange(assigned, dtype=jnp.int32) - starts[sorted_ids]).astype(jnp.int32)
    blocks = assigned // block_len + experts + 1
    row_token = jnp.zeros((blocks * block_len,), jnp.int32).at[target].set((sort_order // per_token).astype(jnp.int32))
    block_expert = jnp.minimum(jnp.searchsorted(ends, jnp.arange(blocks, dtype=jnp.int32) * block_len, side='right'), experts - 1).astype(jnp.int32)
    inputs = normed_in[row_token].reshape(blocks, block_len, normed_in.shape[1])

    def expert_block(pair):
        rows, which = pair
        gate = jnp.dot(rows, w_gate[which], preferred_element_type=jnp.float32)
        upper = jnp.dot(rows, w_up[which], preferred_element_type=jnp.float32)
        hidden = (jax.nn.silu(gate) * upper).astype(jnp.bfloat16)
        return jnp.dot(hidden, w_down[which], preferred_element_type=jnp.float32).astype(jnp.bfloat16)
    outputs = lax.map(expert_block, (inputs, block_expert)).reshape(blocks * block_len, normed_in.shape[1])
    where_row = jnp.zeros((assigned,), jnp.int32).at[sort_order].set(target).reshape(total_tok, per_token)
    expert_share = jnp.exp(expert_logit)
    expert_share = expert_share / lax.optimization_barrier(jnp.sum(expert_share, axis=-1, keepdims=True))
    route_weight = group_weight[:, None] * expert_share
    mixture = tokens_f
    for member in range(per_token):
        mixture = mixture + route_weight[:, member:member + 1] * outputs[where_row[:, member]].astype(jnp.float32)
    residual = mixture.astype(jnp.bfloat16).astype(jnp.float32)
    return normalize(residual, final_gain).astype(jnp.bfloat16)
```

```python
import jax
import jax.numpy as jnp
from jax import lax
from jax.sharding import PartitionSpec as P

D = 2048
CAP = 16
EPS = 1e-06


def local(
    tokens, norm_gain, expert_ids, group_weight, expert_logit, w_gate, w_up, w_down, final_gain
):
    rows, width = tokens.shape
    experts = lax.axis_size("ep")
    slots = experts * CAP
    down_whole = lax.all_gather(w_down, "tp", axis=1, tiled=True)[0]
    both = lax.all_gather(jnp.concatenate((w_gate, w_up), axis=0), "tp", axis=2, tiled=True)
    tokens_f = tokens.astype(jnp.float32)
    inverse_in = lax.rsqrt(jnp.mean(tokens_f * tokens_f, axis=-1, keepdims=True) + EPS)
    normed_in = (tokens_f * inverse_in * norm_gain.astype(jnp.float32)).astype(jnp.bfloat16)
    lane = jnp.arange(experts, dtype=jnp.int32)[None, :]
    first = expert_ids[:, 0:1] == lane
    second = expert_ids[:, 1:2] == lane
    named = (first | second).astype(jnp.bfloat16)
    order = jnp.arange(rows, dtype=jnp.int32)
    earlier = (order[:, None] > order[None, :]).astype(jnp.bfloat16)
    before = jnp.dot(earlier, named, preferred_element_type=jnp.float32)
    rank0 = jnp.sum(jnp.where(first, before, 0.0), axis=1).astype(jnp.int32)
    rank1 = jnp.sum(jnp.where(second, before, 0.0), axis=1).astype(jnp.int32)
    at0 = expert_ids[:, 0] * CAP + rank0
    at1 = expert_ids[:, 1] * CAP + rank1
    slot = jnp.arange(slots, dtype=jnp.int32)
    pick = ((slot[:, None] == at0[None, :]) | (slot[:, None] == at1[None, :])).astype(jnp.bfloat16)
    outgoing = jnp.dot(pick, normed_in, preferred_element_type=jnp.float32).astype(jnp.bfloat16)
    incoming = lax.all_to_all(
        outgoing.reshape(experts, CAP, width), "ep", split_axis=0, concat_axis=0, tiled=True
    )
    routed = incoming.reshape(slots, width)
    gate_full = jnp.dot(routed, both[0], preferred_element_type=jnp.float32)
    up_full = jnp.dot(routed, both[1], preferred_element_type=jnp.float32)
    hidden = (jax.nn.silu(gate_full) * up_full).astype(jnp.bfloat16)
    product = jnp.dot(hidden, down_whole, preferred_element_type=jnp.float32).astype(jnp.bfloat16)
    arrived = lax.all_to_all(
        product.reshape(experts, CAP, width), "ep", split_axis=0, concat_axis=0, tiled=True
    ).reshape(slots, width)
    share = jnp.exp(expert_logit)
    weight = group_weight[:, None] * (share / jnp.sum(share, axis=-1, keepdims=True))
    spread = jnp.where(slot[None, :] == at0[:, None], weight[:, 0:1], 0.0) + jnp.where(
        slot[None, :] == at1[:, None], weight[:, 1:2], 0.0
    )
    high = spread.astype(jnp.bfloat16)
    low = (spread - high.astype(jnp.float32)).astype(jnp.bfloat16)
    mixed = jnp.dot(high, arrived, preferred_element_type=jnp.float32) + jnp.dot(
        low, arrived, preferred_element_type=jnp.float32
    )
    residual = (tokens_f + mixed).astype(jnp.bfloat16)
    pieces = residual.reshape(rows, 4, width // 4).transpose(1, 0, 2)
    sliced = lax.all_to_all(pieces, "tp", split_axis=0, concat_axis=0, tiled=True)
    sliced = sliced.reshape(4 * rows, width // 4).astype(jnp.float32)
    squares = lax.all_gather(jnp.sum(sliced * sliced, axis=-1), "tp", axis=0).sum(axis=0)
    inverse_out = lax.rsqrt(squares / D + EPS)
    return (sliced * inverse_out[:, None] * final_gain.astype(jnp.float32)).astype(jnp.bfloat16)


def solution(mesh):
    placed = (
        P(("ep", "tp"), None),
        P(),
        P(("ep", "tp"), None),
        P(("ep", "tp")),
        P(("ep", "tp"), None),
        P("ep", None, "tp"),
        P("ep", None, "tp"),
        P("ep", "tp", None),
        P("tp"),
    )
    return jax.shard_map(
        local, mesh=mesh, in_specs=placed, out_specs=P("ep", "tp"), check_vma=False
    )
```

```python
import functools

import jax
import jax.numpy as jnp
from jax import lax
from jax.experimental import pallas as pl
from jax.experimental.pallas import tpu as pltpu
from jax.sharding import PartitionSpec as P

D = 2048
FF = 1024
CAP = 16
ROWS = 256
PLANES = 8
GROUP = 8
LANES = GROUP * CAP
TP = 4
EPS = 1e-06
MESH = pl.DeviceIdType.MESH
F32 = jnp.float32
BF16 = jnp.bfloat16


def plane_step(i):
    return 4 + (1 - 2 * (i % 2)) * ((i + 1) // 2)


def kernel(
    tokens, gain, ids, group_weight, logit, w_gate, w_up, w_down, final_gain, out,
    normed, packed, routed, hidden, product, returned, wg, wu, wd, high, low, mixed,
    gains, result, finished,
    own_sem, w_send, w_recv, gain_send, gain_recv, out_send, out_recv, back_send, back_recv,
    last_send, last_recv,
):
    ep, tp = lax.axis_index("ep"), lax.axis_index("tp")
    z, inner = ep // GROUP, ep % GROUP
    x, core = inner // 2, inner % 2
    right, left, opposite = (tp + 1) % TP, (tp + 3) % TP, (tp + 2) % TP

    def peer(i):
        step, j = i // GROUP, (i + 1) % GROUP
        pz = (z + plane_step(step)) % PLANES
        return pz * GROUP + ((x + j // 2) % 4) * 2 + (core + j % 2) % 2

    barrier = pltpu.get_barrier_semaphore()

    def greet(i, _):
        pl.semaphore_signal(barrier, inc=1, device_id={"ep": peer(i), "tp": tp}, device_id_type=MESH)
        return 0

    lax.fori_loop(0, 63, greet, 0)
    for other in (right, left, opposite):
        pl.semaphore_signal(barrier, inc=1, device_id={"ep": ep, "tp": other}, device_id_type=MESH)

    own = [
        pltpu.make_async_copy(w_gate, wg.at[tp], own_sem.at[0]),
        pltpu.make_async_copy(w_up, wu.at[tp], own_sem.at[1]),
        pltpu.make_async_copy(w_down, wd.at[tp], own_sem.at[2]),
    ]
    for copy in own:
        copy.start()

    def norm_rows(i, _):
        at = pl.ds(pl.multiple_of(i * 32, 32), 32)
        t = tokens[at, :].astype(F32)
        inverse = lax.rsqrt(jnp.mean(t * t, axis=-1, keepdims=True) + EPS)
        normed[at, :] = (t * inverse * gain[...].astype(F32)).astype(BF16)
        return 0

    lax.fori_loop(0, ROWS // 32, norm_rows, 0)

    id0, id1 = ids[0:1, :], ids[1:2, :]
    lane = lax.broadcasted_iota(jnp.int32, (PLANES * GROUP, ROWS), 0)
    first, second = lane == id0, lane == id1
    named = jnp.where(first, 1.0, jnp.where(second, 1.0, 0.0)).astype(BF16)
    earlier = jnp.where(
        lax.broadcasted_iota(jnp.int32, (ROWS, ROWS), 0)
        < lax.broadcasted_iota(jnp.int32, (ROWS, ROWS), 1), 1.0, 0.0,
    ).astype(BF16)
    before = jnp.dot(named, earlier, preferred_element_type=F32)
    rank0 = jnp.sum(jnp.where(first, before, 0.0), axis=0, keepdims=True)
    rank1 = jnp.sum(jnp.where(second, before, 0.0), axis=0, keepdims=True)
    at0 = id0.astype(F32) * CAP + rank0
    at1 = id1.astype(F32) * CAP + rank1
    slot = lax.broadcasted_iota(jnp.int32, (LANES, ROWS), 0).astype(F32)

    def pack(p, _):
        base = (p * LANES).astype(F32)
        pick = jnp.where(slot == at0 - base, 1.0, jnp.where(slot == at1 - base, 1.0, 0.0)).astype(BF16)
        for n in range(4):
            rows = jnp.dot(pick, normed[:, n * 512:(n + 1) * 512], preferred_element_type=F32)
            packed[pl.ds(p * GROUP, GROUP), :, n * 512:(n + 1) * 512] = rows.astype(BF16).reshape(GROUP, CAP, 512)
        return 0

    lax.fori_loop(0, PLANES, pack, 0)

    for copy in own:
        copy.wait()
    pl.semaphore_wait(barrier, 66)

    def weights(src, dst, sem, to):
        copy = pltpu.make_async_remote_copy(
            src_ref=src, dst_ref=dst, send_sem=w_send.at[sem], recv_sem=w_recv.at[sem],
            device_id={"ep": ep, "tp": to}, device_id_type=MESH,
        )
        copy.start()
        return copy

    half = FF // TP // 2
    top, bottom = pl.ds(0, half), pl.ds(half, half)
    flights = [
        weights(wg.at[tp], wg.at[tp], 0, right),
        weights(wu.at[tp], wu.at[tp], 1, left),
        weights(wu.at[tp], wu.at[tp], 2, right),
        weights(wg.at[tp], wg.at[tp], 3, left),
    ]

    def dispatch(i, _):
        to = peer(i)
        pltpu.make_async_remote_copy(
            src_ref=packed.at[to], dst_ref=routed.at[ep], send_sem=out_send, recv_sem=out_recv.at[z],
            device_id={"ep": to, "tp": tp}, device_id_type=MESH,
        ).start()
        return 0

    lax.fori_loop(0, 63, dispatch, 0)
    routed[ep] = packed[ep]

    gains[tp] = final_gain[...]
    for k, other in enumerate((right, left, opposite)):
        flights.append(pltpu.make_async_remote_copy(
            src_ref=final_gain, dst_ref=gains.at[tp], send_sem=gain_send.at[k], recv_sem=gain_recv.at[k],
            device_id={"ep": ep, "tp": other}, device_id_type=MESH,
        ))
        flights[-1].start()

    e0, e1 = jnp.exp(logit[0:1, :]), jnp.exp(logit[1:2, :])
    total = e0 + e1
    weight0 = group_weight[...] * (e0 / total)
    weight1 = group_weight[...] * (e1 / total)

    def spread(p, _):
        base = (p * LANES).astype(F32)
        w = jnp.where(slot == at0 - base, weight0, 0.0) + jnp.where(slot == at1 - base, weight1, 0.0)
        w = w.T
        top_term = w.astype(BF16)
        high[p] = top_term
        low[p] = (w - top_term.astype(F32)).astype(BF16)
        return 0

    lax.fori_loop(0, PLANES, spread, 0)

    flights[0].wait_recv()
    flights.append(weights(wg.at[left], wg.at[left], 4, right))
    flights[1].wait_recv()
    flights.append(weights(wu.at[right], wu.at[right], 5, left))
    downs = [
        weights(wd.at[tp, top], wd.at[tp, top], 6, right),
        weights(wd.at[tp, bottom], wd.at[tp, bottom], 7, left),
        weights(wd.at[tp, bottom], wd.at[tp, bottom], 8, right),
        weights(wd.at[tp, top], wd.at[tp, top], 9, left),
    ]
    flights[2].wait_recv()
    flights[3].wait_recv()
    flights[-2].wait_recv()
    flights[-1].wait_recv()

    def rows_of(p, count, dst, sem, at):
        pltpu.make_async_remote_copy(
            src_ref=packed.at[pl.ds(0, count)], dst_ref=dst.at[pl.ds(0, count)], send_sem=out_send,
            recv_sem=sem.at[at], device_id={"ep": ep, "tp": right}, device_id_type=MESH,
        ).wait_recv()

    def expand_plane(p):
        xs = routed[pl.ds(p * GROUP, GROUP)].reshape(LANES, D)

        def piece(q, _):
            g = jnp.dot(xs, wg[q], preferred_element_type=F32)
            u = jnp.dot(xs, wu[q], preferred_element_type=F32)
            hidden[p, q] = (g / (1.0 + jnp.exp(-g)) * u).astype(BF16)
            return 0

        lax.fori_loop(0, TP, piece, 0)

    def expand(i, _):
        p = (z + PLANES - plane_step(i)) % PLANES
        rows_of(p, GROUP, routed, out_recv, p)
        expand_plane(p)
        return 0

    lax.fori_loop(0, 4, expand, 0)
    downs[0].wait_recv()
    downs.append(weights(wd.at[left, top], wd.at[left, top], 10, right))
    downs[1].wait_recv()
    downs.append(weights(wd.at[right, bottom], wd.at[right, bottom], 11, left))
    lax.fori_loop(4, 7, expand, 0)
    rows_of(z, GROUP - 1, routed, out_recv, z)
    expand_plane(z)
    for copy in downs[2:]:
        copy.wait_recv()

    def contract_plane(p):
        for n in range(4):
            cols = slice(n * 512, (n + 1) * 512)
            total_rows = jnp.dot(hidden[p, 0], wd[0, :, cols], preferred_element_type=F32)
            for q in range(1, TP):
                total_rows += jnp.dot(hidden[p, q], wd[q, :, cols], preferred_element_type=F32)
            product[pl.ds(p * GROUP, GROUP), :, cols] = total_rows.astype(BF16).reshape(GROUP, CAP, 512)

    def answer(i, _):
        to = peer(i)
        pltpu.make_async_remote_copy(
            src_ref=product.at[to], dst_ref=returned.at[ep], send_sem=back_send, recv_sem=back_recv.at[z],
            device_id={"ep": to, "tp": tp}, device_id_type=MESH,
        ).start()
        return 0

    def contract(i, _):
        contract_plane((z + PLANES - plane_step(i)) % PLANES)
        return 0

    for begin, end in ((0, 1), (1, 3), (3, 5), (5, 7), (7, 8)):
        lax.fori_loop(begin, end, contract, 0)
        lax.fori_loop(begin * GROUP, min(end * GROUP, 63), answer, 0)
    returned[ep] = product[ep]

    def combine_plane(p):
        rows = returned[pl.ds(p * GROUP, GROUP)].reshape(LANES, D)
        for n in range(4):
            cols = slice(n * 512, (n + 1) * 512)
            mixed[:, cols] += jnp.dot(high[p], rows[:, cols], preferred_element_type=F32) + jnp.dot(
                low[p], rows[:, cols], preferred_element_type=F32
            )

    def combine(i, _):
        p = (z + PLANES - plane_step(i)) % PLANES
        rows_of(p, GROUP, returned, back_recv, p)
        combine_plane(p)
        return 0

    mixed[...] = tokens[...].astype(F32)
    lax.fori_loop(0, 7, combine, 0)
    rows_of(z, GROUP - 1, returned, back_recv, z)
    combine_plane(z)

    for k, copy in enumerate(flights[4:7]):
        copy.wait_recv()

    def close(i, _):
        at = pl.ds(pl.multiple_of(i * 32, 32), 32)
        r = mixed[at, :].astype(BF16).astype(F32)
        inverse = lax.rsqrt(jnp.mean(r * r, axis=-1, keepdims=True) + EPS)
        for n in range(TP):
            result[n, at, :] = (r[:, n * 512:(n + 1) * 512] * inverse * gains[n, 0:1, :]).astype(BF16)
        return 0

    lasts = []
    for part in range(4):
        lax.fori_loop(part * 2, part * 2 + 2, close, 0)
        at = pl.ds(part * 64, 64)
        for k, other in enumerate((right, left, opposite)):
            copy = pltpu.make_async_remote_copy(
                src_ref=result.at[other, at], dst_ref=finished.at[tp, at], send_sem=last_send.at[part, k],
                recv_sem=last_recv.at[part, k], device_id={"ep": ep, "tp": other}, device_id_type=MESH,
            )
            copy.start()
            lasts.append(copy)
    out[tp] = result[tp]
    for copy in lasts:
        copy.wait_recv()
    for other in (right, left, opposite):
        out[other] = finished[other]

    for copy in flights + downs + lasts:
        copy.wait_send()
    for sem, src in ((out_send, packed), (back_send, product)):
        pltpu.make_async_remote_copy(
            src_ref=src.at[pl.ds(0, 63)], dst_ref=routed.at[pl.ds(0, 63)], send_sem=sem, recv_sem=out_recv.at[0],
            device_id={"ep": ep, "tp": right}, device_id_type=MESH,
        ).wait_send()


def local(
    tokens, norm_gain, expert_ids, group_weight, expert_logit, w_gate, w_up, w_down, final_gain
):
    vmem = pl.BlockSpec(memory_space=pltpu.VMEM)
    anywhere = pl.BlockSpec(memory_space=pl.ANY)
    dma, groups = pltpu.SemaphoreType.DMA, PLANES * GROUP
    out = pl.pallas_call(
        kernel,
        out_shape=jax.ShapeDtypeStruct((TP, ROWS, D // TP), BF16),
        in_specs=[vmem] * 5 + [anywhere] * 3 + [vmem],
        out_specs=vmem,
        scratch_shapes=[
            pltpu.VMEM((ROWS, D), BF16),
            pltpu.VMEM((groups, CAP, D), BF16),
            pltpu.VMEM((groups, CAP, D), BF16),
            pltpu.VMEM((PLANES, TP, LANES, FF // TP), BF16),
            pltpu.VMEM((groups, CAP, D), BF16),
            pltpu.VMEM((groups, CAP, D), BF16),
            pltpu.VMEM((TP, D, FF // TP), BF16),
            pltpu.VMEM((TP, D, FF // TP), BF16),
            pltpu.VMEM((TP, FF // TP, D), BF16),
            pltpu.VMEM((PLANES, ROWS, LANES), BF16),
            pltpu.VMEM((PLANES, ROWS, LANES), BF16),
            pltpu.VMEM((ROWS, D), F32),
            pltpu.VMEM((TP, 8, D // TP), F32),
            pltpu.VMEM((TP, ROWS, D // TP), BF16),
            pltpu.VMEM((TP, ROWS, D // TP), BF16),
            dma((3,)), dma((12,)), dma((12,)), dma((3,)), dma((3,)), dma, dma((PLANES,)), dma, dma((PLANES,)),
            dma((4, 3)), dma((4, 3)),
        ],
        compiler_params=pltpu.CompilerParams(
            collective_id=0, has_side_effects=True, vmem_limit_bytes=60 * 1024 * 1024
        ),
    )(
        tokens, norm_gain[None, :], expert_ids.T, group_weight[None, :], expert_logit.T,
        w_gate[0], w_up[0], w_down[0], jnp.broadcast_to(final_gain.astype(F32)[None, :], (8, D // TP)),
    )
    return out.reshape(TP * ROWS, D // TP)


def solution(mesh):
    placed = (
        P(("ep", "tp"), None),
        P(),
        P(("ep", "tp"), None),
        P(("ep", "tp")),
        P(("ep", "tp"), None),
        P("ep", None, "tp"),
        P("ep", None, "tp"),
        P("ep", "tp", None),
        P("tp"),
    )
    return jax.shard_map(
        local, mesh=mesh, in_specs=placed, out_specs=P("ep", "tp"), check_vma=False
    )
```

```python
import jax
import jax.numpy as jnp
from jax import lax
from jax.experimental import pallas as pl
from jax.experimental.pallas import tpu as pltpu
from jax.sharding import PartitionSpec as P

D = 2048
FF = 1024
CAP = 16
ROWS = 256
PLANES = 8
GROUP = 8
LANES = GROUP * CAP
TP = 4
COL = D // TP
EPS = 1e-06
MESH = pl.DeviceIdType.MESH
F32 = jnp.float32
BF16 = jnp.bfloat16

A, B, C, DD, E = 0, 20, 40, 48, 56
BLOCK_A, BLOCK_B, BLOCK_C, BLOCK_D, BLOCK_E = range(5)
AT_E, AT_C, AT_D, AT_A, AT_B, AT_UP, AT_DOWN, AT_FAR = range(8)
LANE = (0, 384, 768, 896, 1024)


def kernel(
    tokens, gain, ids, group_weight, logit, w_gate, w_up, w_down, final_gain, out,
    normed, raw, info, pick, packed, routed, hidden, product, returned, wg, wu, wd, high, low,
    far, far_in, near, near_in, residual, slices, squares, inverse_out, inverses,
    own_sem, w_send, w_recv, d_send, d_recv, info_send, info_recv, raw_send, raw_recv, disp_send, disp_recv,
    ret_send, ret_recv, far_send, far_recv, near_send, near_recv, slice_send, slice_recv, inv_send, inv_recv,
):
    ep, tp = lax.axis_index("ep"), lax.axis_index("tp")
    z, inner = ep // GROUP, ep % GROUP
    up1, down1, up2, down2 = ((z + k) % PLANES for k in (1, 7, 2, 6))
    right, left, opposite = (tp + 1) % TP, (tp + 3) % TP, (tp + 2) % TP

    def remote(src, dst, send, recv, to_z, to_inner, to_tp):
        return pltpu.make_async_remote_copy(
            src_ref=src, dst_ref=dst, send_sem=send, recv_sem=recv,
            device_id={"ep": to_z * GROUP + to_inner, "tp": to_tp}, device_id_type=MESH,
        )

    def landed(dst, recv):
        remote(dst, dst, info_send.at[0], recv, z, inner, right).wait_recv()

    def sent(src, send):
        remote(src, src, send, info_recv.at[0], z, inner, right).wait_send()

    barrier = pltpu.get_barrier_semaphore()

    def greet(to_z, to_inner, to_tp):
        pl.semaphore_signal(
            barrier, inc=1, device_id={"ep": to_z * GROUP + to_inner, "tp": to_tp}, device_id_type=MESH
        )

    def greet_plane(i, _):
        o = i // GROUP
        greet((z + PLANES + (1 - 2 * (o % 2)) * (1 + o // 2)) % PLANES, i % GROUP, tp)
        return 0

    def greet_own(j, _):
        greet(z, (inner + j) % GROUP, tp)
        return 0

    lax.fori_loop(0, 4 * GROUP, greet_plane, 0)
    lax.fori_loop(1, GROUP, greet_own, 0)
    for other in (right, left, opposite):
        greet(z, inner, other)

    own = [
        pltpu.make_async_copy(w_gate, wg.at[tp], own_sem.at[0]),
        pltpu.make_async_copy(w_up, wu.at[tp], own_sem.at[1]),
    ] + [
        pltpu.make_async_copy(w_down.at[:, pl.ds(n * COL, COL)], wd.at[tp, n], own_sem.at[2 + n]) for n in range(TP)
    ]
    for copy in own:
        copy.start()

    def norm_rows(i, _):
        at = pl.ds(pl.multiple_of(i * 32, 32), 32)
        t = tokens[at, :].astype(F32)
        inverse = lax.rsqrt(jnp.mean(t * t, axis=-1, keepdims=True) + EPS)
        t = (t * inverse * gain[...].astype(F32)).astype(BF16)
        for n in range(TP):
            normed[n, at, :] = t[:, n * COL:(n + 1) * COL]
        return 0

    lax.fori_loop(0, ROWS // 32, norm_rows, 0)

    id0, id1 = ids[0:1, :], ids[1:2, :]
    lane = lax.broadcasted_iota(jnp.int32, (PLANES * GROUP, ROWS), 0)
    first, second = lane == id0, lane == id1
    named = jnp.where(first, 1.0, jnp.where(second, 1.0, 0.0)).astype(BF16)
    earlier = jnp.where(
        lax.broadcasted_iota(jnp.int32, (ROWS, ROWS), 0)
        < lax.broadcasted_iota(jnp.int32, (ROWS, ROWS), 1), 1.0, 0.0,
    ).astype(BF16)
    before = jnp.dot(named, earlier, preferred_element_type=F32)
    e0, e1 = jnp.exp(logit[0:1, :]), jnp.exp(logit[1:2, :])
    total = e0 + e1
    info[BLOCK_E, 0:1, :] = id0.astype(F32) * CAP + jnp.sum(jnp.where(first, before, 0.0), axis=0, keepdims=True)
    info[BLOCK_E, 1:2, :] = id1.astype(F32) * CAP + jnp.sum(jnp.where(second, before, 0.0), axis=0, keepdims=True)
    info[BLOCK_E, 2:3, :] = group_weight[...] * (e0 / total)
    info[BLOCK_E, 3:4, :] = group_weight[...] * (e1 / total)
    info[BLOCK_E, 4:8, :] = jnp.zeros((4, ROWS), F32)

    sections = {
        BLOCK_A: ((0, 128, z * LANES), (128, 128, up1 * LANES), (256, 64, up2 * LANES)),
        BLOCK_B: ((0, 128, z * LANES), (128, 128, down1 * LANES), (256, 64, down2 * LANES + 64)),
        BLOCK_C: ((0, 128, z * LANES),),
        BLOCK_D: ((0, 128, z * LANES),),
        BLOCK_E: ((0, 128, z * LANES),),
    }
    first_group = {BLOCK_A: A, BLOCK_B: B, BLOCK_C: C, BLOCK_D: DD, BLOCK_E: E}

    def make_pick(block):
        at0, at1 = info[block, 0:1, :], info[block, 1:2, :]
        for start, count, number in sections[block]:
            slot = (lax.broadcasted_iota(jnp.int32, (count, ROWS), 0) + number).astype(F32)
            row = first_group[block] * CAP + start
            pick[row:row + count, :] = jnp.where(slot == at0, 1.0, jnp.where(slot == at1, 1.0, 0.0)).astype(BF16)

    def make_weights(block):
        at0, at1, w0, w1 = (info[block, k:k + 1, :] for k in range(4))
        for start, count, number in sections[block]:
            slot = (lax.broadcasted_iota(jnp.int32, (128, ROWS), 0) + number).astype(F32)
            w = (jnp.where(slot == at0, w0, 0.0) + jnp.where(slot == at1, w1, 0.0)).T[:, :count]
            top_term = w.astype(BF16)
            lanes = slice(LANE[block] + start, LANE[block] + start + count)
            high[:, lanes] = top_term
            low[:, lanes] = (w - top_term.astype(F32)).astype(BF16)

    def pack(block, groups, src, n):
        row = first_group[block] * CAP
        rows = jnp.dot(pick[row:row + groups * CAP, :], src, preferred_element_type=F32).astype(BF16)
        packed[pl.ds(first_group[block], groups), :, pl.ds(pl.multiple_of(n * COL, COL), COL)] = rows.reshape(
            groups, CAP, COL
        )

    def send_own_plane(block, at):
        base = first_group[block]

        def send(j, _):
            to = (inner + j) % GROUP
            remote(packed.at[base + to], routed.at[at * GROUP + inner], disp_send, disp_recv.at[at], z, to, tp).start()
            return 0

        lax.fori_loop(1, GROUP, send, 0)
        routed[at * GROUP + inner] = packed[base + inner]

    make_pick(BLOCK_E)
    for copy in own:
        copy.wait()
    pl.semaphore_wait(barrier, 42)

    def hop_out(n, _):
        remote(normed.at[n], raw.at[0, n], raw_send, raw_recv.at[0, n], up1, inner, tp).start()
        remote(normed.at[n], raw.at[1, n], raw_send, raw_recv.at[1, n], down1, inner, tp).start()
        return 0

    tells = [
        remote(info.at[BLOCK_E], info.at[block], info_send.at[block], info_recv.at[block], to, inner, tp)
        for block, to in ((BLOCK_C, up1), (BLOCK_D, down1), (BLOCK_A, up2), (BLOCK_B, down2))
    ]
    for copy in tells:
        copy.start()
    lax.fori_loop(0, TP, hop_out, 0)

    def weights(src, dst, k, to):
        copy = remote(src, dst, w_send.at[k], w_recv.at[k], z, inner, to)
        copy.start()
        return copy

    flights = [
        weights(wg.at[tp], wg.at[tp], 0, right),
        weights(wu.at[tp], wu.at[tp], 1, left),
        weights(wu.at[tp], wu.at[tp], 2, right),
        weights(wg.at[tp], wg.at[tp], 3, left),
    ]

    def pack_own(n, _):
        pack(BLOCK_E, 8, normed[n], n)
        return 0

    lax.fori_loop(0, TP, pack_own, 0)
    send_own_plane(BLOCK_E, AT_E)
    for copy in tells:
        copy.wait_recv()
    for block in (BLOCK_C, BLOCK_D, BLOCK_A, BLOCK_B):
        make_pick(block)

    def hop_on(n, _):
        landed(raw.at[0, n], raw_recv.at[0, n])
        remote(raw.at[0, n], raw.at[2, n], raw_send, raw_recv.at[2, n], up1, inner, tp).start()
        landed(raw.at[1, n], raw_recv.at[1, n])
        remote(raw.at[1, n], raw.at[3, n], raw_send, raw_recv.at[3, n], down1, inner, tp).start()
        pack(BLOCK_C, 8, raw[0, n], n)
        pack(BLOCK_D, 8, raw[1, n], n)
        return 0

    lax.fori_loop(0, TP, hop_on, 0)
    send_own_plane(BLOCK_C, AT_C)
    send_own_plane(BLOCK_D, AT_D)

    half = FF // TP // 2
    top, bottom = pl.ds(0, half), pl.ds(half, half)

    def down_out(n):
        return [
            remote(wd.at[tp, n], wd.at[tp, n], d_send.at[n, 0], d_recv.at[n, 0], z, inner, right),
            remote(wd.at[tp, n], wd.at[tp, n], d_send.at[n, 1], d_recv.at[n, 1], z, inner, left),
        ]

    def down_on(n):
        return [
            remote(wd.at[left, n, top], wd.at[left, n, top], d_send.at[n, 2], d_recv.at[n, 2], z, inner, right),
            remote(wd.at[right, n, bottom], wd.at[right, n, bottom], d_send.at[n, 3], d_recv.at[n, 3], z, inner, left),
        ]

    def start(copies):
        for copy in copies:
            copy.start()

    flights[0].wait_recv()
    flights.append(weights(wg.at[left], wg.at[left], 4, right))
    flights[1].wait_recv()
    flights.append(weights(wu.at[right], wu.at[right], 5, left))
    outs, ons = [down_out(n) for n in range(TP)], [down_on(n) for n in range(TP)]
    start(outs[0])
    start(outs[1])

    def relay_down(n):
        for copy in outs[n]:
            copy.wait_recv()
        start(ons[n])
        if n + 2 < TP:
            start(outs[n + 2])

    def hop_last(n, _):
        landed(raw.at[2, n], raw_recv.at[2, n])
        landed(raw.at[3, n], raw_recv.at[3, n])
        pack(BLOCK_A, 20, raw[2, n], n)
        pack(BLOCK_B, 20, raw[3, n], n)
        cols = pl.ds(pl.multiple_of(n * COL, COL), COL)

        def send_next(i, _):
            remote(
                packed.at[A + 8 + i, :, cols], routed.at[AT_UP * GROUP + inner, :, cols], disp_send,
                disp_recv.at[AT_UP], up1, i, tp,
            ).start()
            remote(
                packed.at[B + 8 + i, :, cols], routed.at[AT_DOWN * GROUP + inner, :, cols], disp_send,
                disp_recv.at[AT_DOWN], down1, i, tp,
            ).start()
            return 0

        def send_far(i, _):
            remote(
                packed.at[A + 16 + i, :, cols], routed.at[AT_FAR * GROUP + inner, :, cols], disp_send,
                disp_recv.at[AT_FAR], up2, i, tp,
            ).start()
            remote(
                packed.at[B + 16 + i, :, cols], routed.at[AT_FAR * GROUP + inner, :, cols], disp_send,
                disp_recv.at[AT_FAR], down2, 4 + i, tp,
            ).start()
            return 0

        lax.fori_loop(0, 4, send_far, 0)
        lax.fori_loop(0, GROUP, send_next, 0)
        return 0

    lax.fori_loop(0, TP, hop_last, 0)
    send_own_plane(BLOCK_A, AT_A)
    send_own_plane(BLOCK_B, AT_B)

    for block in range(5):
        make_weights(block)

    def expand(q, first_row, count):
        groups = count // CAP
        xs = routed[pl.ds(first_row // CAP, groups)].reshape(count, D)
        g = jnp.dot(xs, wg[q], preferred_element_type=F32)
        u = jnp.dot(xs, wu[q], preferred_element_type=F32)
        hidden[q, pl.ds(first_row, count), :] = (g / (1.0 + jnp.exp(-g)) * u).astype(BF16)

    def expand_near(q):
        def part(i, _):
            expand(q, pl.multiple_of(i * 320, 320), 320)
            return 0

        lax.fori_loop(0, 2, part, 0)

    def expand_all(first_row, count):
        def part(q, _):
            expand(q, first_row, count)
            return 0

        lax.fori_loop(0, TP, part, 0)

    def rows_landed(at, groups):
        landed(routed.at[pl.ds(0, groups)], disp_recv.at[at])

    for at in (AT_E, AT_C, AT_D, AT_A, AT_B):
        rows_landed(at, GROUP - 1)
    expand_near(tp)
    flights[2].wait_recv()
    flights[3].wait_recv()
    expand_near(left)
    expand_near(right)
    flights[4].wait_recv()
    flights[5].wait_recv()
    expand_near(opposite)
    relay_down(0)
    rows_landed(AT_UP, GROUP)
    rows_landed(AT_DOWN, GROUP)
    expand_all(640, 256)
    relay_down(1)
    rows_landed(AT_FAR, GROUP)
    expand_all(896, 128)

    some = (tp + 3) // 4

    def columns_at(k):
        if k < 3:
            return k + some * ((4 + k - tp) // 4)
        return tp + (1 - some) * 3

    upper = inner // 4

    def contract(k):
        n = columns_at(k)
        landed(wd.at[opposite, 0, top], d_recv.at[n, 2])
        landed(wd.at[opposite, 0, bottom], d_recv.at[n, 3])

        def part(i, _):
            at = pl.ds(pl.multiple_of(i * 256, 256), 256)
            rows = jnp.dot(hidden[0, at, :], wd[0, n], preferred_element_type=F32)
            for q in range(1, TP):
                rows += jnp.dot(hidden[q, at, :], wd[q, n], preferred_element_type=F32)
            product[k, pl.ds(i * 16, 16)] = rows.astype(BF16).reshape(16, CAP, COL)
            return 0

        lax.fori_loop(0, 4, part, 0)

        def answer(at, group, block, to_z, i):
            remote(
                product.at[k, at * GROUP + i], returned.at[k, group], ret_send, ret_recv.at[block, k], to_z, i, tp
            ).start()

        def send_far(i, _):
            answer(AT_FAR, 16 + inner + 16 * upper, upper, (z + 6 + 4 * upper) % PLANES, i)
            answer(AT_UP, A + 8 + inner, BLOCK_A, down1, i)
            answer(AT_DOWN, B + 8 + inner, BLOCK_B, up1, i)
            return 0

        ways = ((AT_A, BLOCK_A), (AT_B, BLOCK_B), (AT_C, BLOCK_C), (AT_D, BLOCK_D), (AT_E, BLOCK_E))

        def send_own(j, _):
            to = (inner + j) % GROUP
            for at, block in ways:
                answer(at, first_group[block] + inner, block, z, to)
            return 0

        lax.fori_loop(0, GROUP, send_far, 0)
        lax.fori_loop(1, GROUP, send_own, 0)
        for at, block in ways:
            returned[k, first_group[block] + inner] = product[k, at * GROUP + inner]

    def weighed(block, groups, k):
        remotes = groups - 1
        landed(returned.at[k, pl.ds(0, remotes)], ret_recv.at[block, k])
        rows = returned[k, pl.ds(first_group[block], groups)].reshape(groups * CAP, COL)
        lanes = slice(LANE[block], LANE[block] + groups * CAP)
        return jnp.dot(high[:, lanes], rows, preferred_element_type=F32) + jnp.dot(
            low[:, lanes], rows, preferred_element_type=F32
        )

    def send_partials(k):
        far[0, k] = weighed(BLOCK_A, 20, k).astype(BF16)
        remote(far.at[0, k], far_in.at[0, k], far_send, far_recv.at[0, k], down1, inner, tp).start()
        far[1, k] = weighed(BLOCK_B, 20, k).astype(BF16)
        remote(far.at[1, k], far_in.at[1, k], far_send, far_recv.at[1, k], up1, inner, tp).start()

    def add_partials(k):
        for side, block, to in ((0, BLOCK_C, down1), (1, BLOCK_D, up1)):
            here = weighed(block, 8, k)
            landed(far_in.at[side, k], far_recv.at[side, k])
            near[side, k] = (here + far_in[side, k].astype(F32)).astype(BF16)
            remote(near.at[side, k], near_in.at[side, k], near_send, near_recv.at[side, k], to, inner, tp).start()

    def close(k):
        n = columns_at(k)
        here = weighed(BLOCK_E, 8, k)
        landed(near_in.at[0, k], near_recv.at[0, k])
        landed(near_in.at[1, k], near_recv.at[1, k])
        t = tokens[:, pl.ds(pl.multiple_of(n * COL, COL), COL)].astype(F32)
        r = (t + here + near_in[0, k].astype(F32) + near_in[1, k].astype(F32)).astype(BF16)
        residual[k] = r
        s = r.astype(F32)
        s = s * s
        s = s[:, 0:128] + s[:, 128:256] + s[:, 256:384] + s[:, 384:512]
        squares[...] = s if k == 0 else squares[...] + s

        @pl.when(n != tp)
        def _():
            remote(residual.at[k], slices.at[tp], slice_send, slice_recv.at[tp], z, inner, n).start()

        @pl.when(n == tp)
        def _():
            slices[tp] = residual[k]

    contract(0)
    relay_down(2)
    contract(1)
    send_partials(0)
    relay_down(3)
    contract(2)
    send_partials(1)
    add_partials(0)
    contract(3)
    send_partials(2)
    add_partials(1)
    close(0)
    send_partials(3)
    add_partials(2)
    close(1)
    add_partials(3)
    close(2)
    close(3)

    inverse = lax.rsqrt(jnp.sum(squares[...], axis=-1, keepdims=True) / D + EPS)
    inverse_out[...] = jnp.broadcast_to(inverse, (ROWS, 128)).T[0:8, :]
    lasts = [
        remote(inverse_out, inverses.at[tp], inv_send.at[k], inv_recv.at[k], z, inner, other)
        for k, other in enumerate((right, left, opposite))
    ]
    start(lasts)
    inverses[tp] = inverse_out[...]

    def finish(source):
        column = jnp.broadcast_to(inverses[source, 0:1, :], (128, ROWS)).T[:, 0:1]
        out[source] = (slices[source].astype(F32) * column * final_gain[...]).astype(BF16)

    finish(tp)
    for copy in lasts:
        copy.wait_recv()
    for other in (right, left, opposite):
        landed(slices.at[other], slice_recv.at[other])
        finish(other)

    for copy in tells + flights + lasts + sum(outs, []) + sum(ons, []):
        copy.wait_send()
    sent(raw, raw_send)
    sent(routed.at[pl.ds(0, 59)], disp_send)
    sent(routed.at[pl.ds(0, 59)], ret_send)
    sent(far, far_send)
    sent(near, near_send)
    sent(slices.at[pl.ds(0, 3)], slice_send)


def local(
    tokens, norm_gain, expert_ids, group_weight, expert_logit, w_gate, w_up, w_down, final_gain
):
    vmem = pl.BlockSpec(memory_space=pltpu.VMEM)
    anywhere = pl.BlockSpec(memory_space=pl.ANY)
    dma, groups = pltpu.SemaphoreType.DMA, PLANES * GROUP
    out = pl.pallas_call(
        kernel,
        out_shape=jax.ShapeDtypeStruct((TP, ROWS, COL), BF16),
        in_specs=[vmem] * 5 + [anywhere] * 3 + [vmem],
        out_specs=vmem,
        scratch_shapes=[
            pltpu.VMEM((TP, ROWS, COL), BF16),
            pltpu.VMEM((4, TP, ROWS, COL), BF16),
            pltpu.VMEM((5, 8, ROWS), F32),
            pltpu.VMEM((groups * CAP, ROWS), BF16),
            pltpu.VMEM((groups, CAP, D), BF16),
            pltpu.VMEM((groups, CAP, D), BF16),
            pltpu.VMEM((TP, groups * CAP, FF // TP), BF16),
            pltpu.VMEM((TP, groups, CAP, COL), BF16),
            pltpu.VMEM((TP, groups, CAP, COL), BF16),
            pltpu.VMEM((TP, D, FF // TP), BF16),
            pltpu.VMEM((TP, D, FF // TP), BF16),
            pltpu.VMEM((TP, TP, FF // TP, COL), BF16),
            pltpu.VMEM((ROWS, 1152), BF16),
            pltpu.VMEM((ROWS, 1152), BF16),
            pltpu.VMEM((2, TP, ROWS, COL), BF16),
            pltpu.VMEM((2, TP, ROWS, COL), BF16),
            pltpu.VMEM((2, TP, ROWS, COL), BF16),
            pltpu.VMEM((2, TP, ROWS, COL), BF16),
            pltpu.VMEM((TP, ROWS, COL), BF16),
            pltpu.VMEM((TP, ROWS, COL), BF16),
            pltpu.VMEM((ROWS, 128), F32),
            pltpu.VMEM((8, ROWS), F32),
            pltpu.VMEM((TP, 8, ROWS), F32),
            dma((6,)), dma((6,)), dma((6,)), dma((TP, 4)), dma((TP, 4)), dma((4,)), dma((4,)), dma, dma((4, TP)),
            dma, dma((PLANES,)), dma, dma((5, TP)), dma, dma((2, TP)), dma, dma((2, TP)), dma, dma((TP,)),
            dma((3,)), dma((3,)),
        ],
        compiler_params=pltpu.CompilerParams(
            collective_id=0, has_side_effects=True, vmem_limit_bytes=62 * 1024 * 1024
        ),
    )(
        tokens, norm_gain[None, :], expert_ids.T, group_weight[None, :], expert_logit.T,
        w_gate[0], w_up[0], w_down[0], final_gain.astype(F32)[None, :],
    )
    return out.reshape(TP * ROWS, COL)


def solution(mesh):
    placed = (
        P(("ep", "tp"), None),
        P(),
        P(("ep", "tp"), None),
        P(("ep", "tp")),
        P(("ep", "tp"), None),
        P("ep", None, "tp"),
        P("ep", None, "tp"),
        P("ep", "tp", None),
        P("tp"),
    )
    return jax.shard_map(
        local, mesh=mesh, in_specs=placed, out_specs=P("ep", "tp"), check_vma=False
    )
```

```python
import jax
import jax.numpy as jnp
from jax import lax
from jax.experimental import pallas as pl
from jax.experimental.pallas import tpu as pltpu
from jax.sharding import PartitionSpec as P

D = 2048
FF = 1024
CAP = 16
ROWS = 256
PLANES = 8
GROUP = 8
LANES = GROUP * CAP
TP = 4
COL = D // TP
EPS = 1e-06
MESH = pl.DeviceIdType.MESH
F32 = jnp.float32
BF16 = jnp.bfloat16

A, B, C, DD, E = 0, 20, 40, 48, 56
BLOCK_A, BLOCK_B, BLOCK_C, BLOCK_D, BLOCK_E = range(5)
AT_E, AT_C, AT_D, AT_A, AT_B, AT_UP, AT_DOWN, AT_FAR = range(8)
LANE = (0, 384, 768, 896, 1024)


def kernel(
    tokens, gain, ids, group_weight, logit, w_gate, w_up, w_down, final_gain, out,
    normed, raw, info, pick, packed, routed, hidden, product, returned, wg, wu, wd, high, low,
    far, far_in, near, near_in, residual, slices, squares, inverse_out, inverses,
    own_sem, w_send, w_recv, d_send, d_recv, info_send, info_recv, raw_send, raw_recv, disp_send, disp_recv,
    ret_send, ret_recv, far_send, far_recv, near_send, near_recv, slice_send, slice_recv, inv_send, inv_recv,
):
    ep, tp = lax.axis_index("ep"), lax.axis_index("tp")
    z, inner = ep // GROUP, ep % GROUP
    up1, down1, up2, down2 = ((z + k) % PLANES for k in (1, 7, 2, 6))
    right, left, opposite = (tp + 1) % TP, (tp + 3) % TP, (tp + 2) % TP

    def remote(src, dst, send, recv, to_z, to_inner, to_tp):
        return pltpu.make_async_remote_copy(
            src_ref=src, dst_ref=dst, send_sem=send, recv_sem=recv,
            device_id={"ep": to_z * GROUP + to_inner, "tp": to_tp}, device_id_type=MESH,
        )

    def landed(dst, recv):
        remote(dst, dst, info_send.at[0], recv, z, inner, right).wait_recv()

    def sent(src, send):
        remote(src, src, send, info_recv.at[0], z, inner, right).wait_send()

    barrier = pltpu.get_barrier_semaphore()

    def greet(to_z, to_inner, to_tp):
        pl.semaphore_signal(
            barrier, inc=1, device_id={"ep": to_z * GROUP + to_inner, "tp": to_tp}, device_id_type=MESH
        )

    def greet_plane(i, _):
        o = i // GROUP
        greet((z + PLANES + (1 - 2 * (o % 2)) * (1 + o // 2)) % PLANES, i % GROUP, tp)
        return 0

    def greet_own(j, _):
        greet(z, (inner + j) % GROUP, tp)
        return 0

    lax.fori_loop(0, 4 * GROUP, greet_plane, 0)
    lax.fori_loop(1, GROUP, greet_own, 0)
    for other in (right, left, opposite):
        greet(z, inner, other)

    own = [
        pltpu.make_async_copy(w_gate, wg.at[tp], own_sem.at[0]),
        pltpu.make_async_copy(w_up, wu.at[tp], own_sem.at[1]),
    ] + [
        pltpu.make_async_copy(w_down.at[:, pl.ds(n * COL, COL)], wd.at[tp, n], own_sem.at[2 + n]) for n in range(TP)
    ]
    for copy in own:
        copy.start()

    def norm_rows(i, _):
        at = pl.ds(pl.multiple_of(i * 32, 32), 32)
        t = tokens[at, :].astype(F32)
        inverse = lax.rsqrt(jnp.mean(t * t, axis=-1, keepdims=True) + EPS)
        t = (t * inverse * gain[...].astype(F32)[None, :]).astype(BF16)
        for n in range(TP):
            normed[n, at, :] = t[:, n * COL:(n + 1) * COL]
        return 0

    lax.fori_loop(0, ROWS // 32, norm_rows, 0)

    id0, id1 = ids[0:1, :], ids[1:2, :]
    lane = lax.broadcasted_iota(jnp.int32, (PLANES * GROUP, ROWS), 0)
    first, second = lane == id0, lane == id1
    named = jnp.where(first, 1.0, jnp.where(second, 1.0, 0.0)).astype(BF16)
    earlier = jnp.where(
        lax.broadcasted_iota(jnp.int32, (ROWS, ROWS), 0)
        < lax.broadcasted_iota(jnp.int32, (ROWS, ROWS), 1), 1.0, 0.0,
    ).astype(BF16)
    before = jnp.dot(named, earlier, preferred_element_type=F32)
    e0, e1 = jnp.exp(logit[0:1, :]), jnp.exp(logit[1:2, :])
    total = e0 + e1
    info[BLOCK_E, 0:1, :] = id0.astype(F32) * CAP + jnp.sum(jnp.where(first, before, 0.0), axis=0, keepdims=True)
    info[BLOCK_E, 1:2, :] = id1.astype(F32) * CAP + jnp.sum(jnp.where(second, before, 0.0), axis=0, keepdims=True)
    info[BLOCK_E, 2:3, :] = group_weight[...] * (e0 / total)
    info[BLOCK_E, 3:4, :] = group_weight[...] * (e1 / total)
    info[BLOCK_E, 4:8, :] = jnp.zeros((4, ROWS), F32)

    sections = {
        BLOCK_A: ((0, 128, z * LANES), (128, 128, up1 * LANES), (256, 64, up2 * LANES)),
        BLOCK_B: ((0, 128, z * LANES), (128, 128, down1 * LANES), (256, 64, down2 * LANES + 64)),
        BLOCK_C: ((0, 128, z * LANES),),
        BLOCK_D: ((0, 128, z * LANES),),
        BLOCK_E: ((0, 128, z * LANES),),
    }
    first_group = {BLOCK_A: A, BLOCK_B: B, BLOCK_C: C, BLOCK_D: DD, BLOCK_E: E}

    def make_pick(block):
        at0, at1 = info[block, 0:1, :], info[block, 1:2, :]
        for start, count, number in sections[block]:
            slot = (lax.broadcasted_iota(jnp.int32, (count, ROWS), 0) + number).astype(F32)
            row = first_group[block] * CAP + start
            pick[row:row + count, :] = jnp.where(slot == at0, 1.0, jnp.where(slot == at1, 1.0, 0.0)).astype(BF16)

    def make_weights(block):
        at0, at1, w0, w1 = (info[block, k:k + 1, :] for k in range(4))
        for start, count, number in sections[block]:
            slot = (lax.broadcasted_iota(jnp.int32, (128, ROWS), 0) + number).astype(F32)
            w = (jnp.where(slot == at0, w0, 0.0) + jnp.where(slot == at1, w1, 0.0)).T[:, :count]
            top_term = w.astype(BF16)
            lanes = slice(LANE[block] + start, LANE[block] + start + count)
            high[:, lanes] = top_term
            low[:, lanes] = (w - top_term.astype(F32)).astype(BF16)

    def pack(block, groups, src, n):
        row = first_group[block] * CAP
        rows = jnp.dot(pick[row:row + groups * CAP, :], src, preferred_element_type=F32).astype(BF16)
        packed[pl.ds(first_group[block], groups), :, pl.ds(pl.multiple_of(n * COL, COL), COL)] = rows.reshape(
            groups, CAP, COL
        )

    def send_own_plane(ways, n):
        cols = pl.ds(pl.multiple_of(n * COL, COL), COL)

        def send(j, _):
            to = (inner + j) % GROUP
            for block, at in ways:
                remote(
                    packed.at[first_group[block] + to, :, cols], routed.at[at * GROUP + inner, :, cols], disp_send,
                    disp_recv.at[at], z, to, tp,
                ).start()
            return 0

        lax.fori_loop(1, GROUP, send, 0)
        for block, at in ways:
            routed[at * GROUP + inner, :, cols] = packed[first_group[block] + inner, :, cols]

    make_pick(BLOCK_E)
    for copy in own:
        copy.wait()
    pl.semaphore_wait(barrier, 42)

    def hop_out(n, _):
        remote(normed.at[n], raw.at[0, n], raw_send, raw_recv.at[0, n], up1, inner, tp).start()
        remote(normed.at[n], raw.at[1, n], raw_send, raw_recv.at[1, n], down1, inner, tp).start()
        return 0

    tells = [
        remote(info.at[BLOCK_E], info.at[block], info_send.at[block], info_recv.at[block], to, inner, tp)
        for block, to in ((BLOCK_C, up1), (BLOCK_D, down1), (BLOCK_A, up2), (BLOCK_B, down2))
    ]
    for copy in tells:
        copy.start()
    lax.fori_loop(0, TP, hop_out, 0)

    def weights(src, dst, k, to):
        copy = remote(src, dst, w_send.at[k], w_recv.at[k], z, inner, to)
        copy.start()
        return copy

    flights = [
        weights(wg.at[tp], wg.at[tp], 0, right),
        weights(wu.at[tp], wu.at[tp], 1, left),
        weights(wu.at[tp], wu.at[tp], 2, right),
        weights(wg.at[tp], wg.at[tp], 3, left),
    ]

    def pack_own(n, _):
        pack(BLOCK_E, 8, normed[n], n)
        send_own_plane(((BLOCK_E, AT_E),), n)
        return 0

    lax.fori_loop(0, TP, pack_own, 0)
    for copy in tells:
        copy.wait_recv()
    for block in (BLOCK_C, BLOCK_D, BLOCK_A, BLOCK_B):
        make_pick(block)

    def hop_on(n, _):
        landed(raw.at[0, n], raw_recv.at[0, n])
        remote(raw.at[0, n], raw.at[2, n], raw_send, raw_recv.at[2, n], up1, inner, tp).start()
        landed(raw.at[1, n], raw_recv.at[1, n])
        remote(raw.at[1, n], raw.at[3, n], raw_send, raw_recv.at[3, n], down1, inner, tp).start()
        pack(BLOCK_C, 8, raw[0, n], n)
        pack(BLOCK_D, 8, raw[1, n], n)
        send_own_plane(((BLOCK_C, AT_C), (BLOCK_D, AT_D)), n)
        return 0

    lax.fori_loop(0, TP, hop_on, 0)

    half = FF // TP // 2
    top, bottom = pl.ds(0, half), pl.ds(half, half)

    def over_y(q, n, part, k, to):
        return remote(wd.at[q, n, part], wd.at[q, n, part], d_send.at[n, k], d_recv.at[n, k], z, inner, to)

    def down_out(n):
        return [
            over_y(tp, n, top, 0, right), over_y(tp, n, bottom, 1, left),
            over_y(tp, n, bottom, 4, right), over_y(tp, n, top, 5, left),
        ]

    def down_on(n):
        return [over_y(left, n, top, 2, right), over_y(right, n, bottom, 3, left)]

    def start(copies):
        for copy in copies:
            copy.start()

    flights[0].wait_recv()
    flights.append(weights(wg.at[left], wg.at[left], 4, right))
    flights[1].wait_recv()
    flights.append(weights(wu.at[right], wu.at[right], 5, left))
    outs, ons = [down_out(n) for n in (0, 2, 3, 1)], [down_on(n) for n in (0, 2, 3, 1)]
    start(outs[0])

    def relay_down(k):
        outs[k][0].wait_recv()
        outs[k][1].wait_recv()
        start(ons[k])
        if k + 1 < TP:
            start(outs[k + 1])

    def expand(q, first_row, count):
        groups = count // CAP
        xs = routed[pl.ds(first_row // CAP, groups)].reshape(count, D)
        g = jnp.dot(xs, wg[q], preferred_element_type=F32)
        u = jnp.dot(xs, wu[q], preferred_element_type=F32)
        hidden[q, pl.ds(first_row, count), :] = (g / (1.0 + jnp.exp(-g)) * u).astype(BF16)

    def expand_of(order, first_row, count):
        def part(i, _):
            expand((tp + order[0] + order[1] * i) % TP, first_row, count)
            return 0

        lax.fori_loop(0, order[2], part, 0)

    def rows_landed(at, groups):
        landed(routed.at[pl.ds(0, groups)], disp_recv.at[at])

    for block in range(5):
        make_weights(block)
    rows_landed(AT_E, GROUP - 1)
    rows_landed(AT_C, GROUP - 1)
    rows_landed(AT_D, GROUP - 1)
    expand_of((0, 0, 1), 0, 384)

    def hop_last(n, _):
        landed(raw.at[2, n], raw_recv.at[2, n])
        landed(raw.at[3, n], raw_recv.at[3, n])
        pack(BLOCK_A, 20, raw[2, n], n)
        pack(BLOCK_B, 20, raw[3, n], n)
        send_own_plane(((BLOCK_A, AT_A), (BLOCK_B, AT_B)), n)
        cols = pl.ds(pl.multiple_of(n * COL, COL), COL)

        def send_next(i, _):
            remote(
                packed.at[A + 8 + i, :, cols], routed.at[AT_UP * GROUP + inner, :, cols], disp_send,
                disp_recv.at[AT_UP], up1, i, tp,
            ).start()
            remote(
                packed.at[B + 8 + i, :, cols], routed.at[AT_DOWN * GROUP + inner, :, cols], disp_send,
                disp_recv.at[AT_DOWN], down1, i, tp,
            ).start()
            return 0

        def send_far(i, _):
            remote(
                packed.at[A + 16 + i, :, cols], routed.at[AT_FAR * GROUP + inner, :, cols], disp_send,
                disp_recv.at[AT_FAR], up2, i, tp,
            ).start()
            remote(
                packed.at[B + 16 + i, :, cols], routed.at[AT_FAR * GROUP + inner, :, cols], disp_send,
                disp_recv.at[AT_FAR], down2, 4 + i, tp,
            ).start()
            return 0

        lax.fori_loop(0, 4, send_far, 0)
        lax.fori_loop(0, GROUP, send_next, 0)
        return 0

    lax.fori_loop(0, TP, hop_last, 0)

    flights[2].wait_recv()
    flights[3].wait_recv()
    expand_of((1, 2, 2), 0, 384)
    rows_landed(AT_A, GROUP - 1)
    rows_landed(AT_B, GROUP - 1)
    expand_of((3, 1, 3), 384, 256)
    flights[4].wait_recv()
    flights[5].wait_recv()
    expand_of((2, 0, 1), 0, 640)
    relay_down(0)
    rows_landed(AT_UP, GROUP)
    rows_landed(AT_DOWN, GROUP)
    rows_landed(AT_FAR, GROUP)
    expand_of((0, 1, 4), 640, 384)

    def columns_at(k):
        last = tp // 3
        return (0, 2, 3 - 2 * last, 1 + 2 * last)[k]

    upper = inner // 4

    def contract(k):
        n = columns_at(k)
        for sem in range(2, 6):
            landed(wd.at[opposite, 0, top], d_recv.at[n, sem])

        def part(i, _):
            at = pl.ds(pl.multiple_of(i * 256, 256), 256)
            rows = jnp.dot(hidden[0, at, :], wd[0, n], preferred_element_type=F32)
            for q in range(1, TP):
                rows += jnp.dot(hidden[q, at, :], wd[q, n], preferred_element_type=F32)
            product[k, pl.ds(i * 16, 16)] = rows.astype(BF16).reshape(16, CAP, COL)
            return 0

        lax.fori_loop(0, 4, part, 0)

        def answer(at, group, block, to_z, i):
            remote(
                product.at[k, at * GROUP + i], returned.at[k, group], ret_send, ret_recv.at[block, k], to_z, i, tp
            ).start()

        def send_far(i, _):
            answer(AT_FAR, 16 + inner + 16 * upper, upper, (z + 6 + 4 * upper) % PLANES, i)
            answer(AT_UP, A + 8 + inner, BLOCK_A, down1, i)
            answer(AT_DOWN, B + 8 + inner, BLOCK_B, up1, i)
            return 0

        ways = ((AT_A, BLOCK_A), (AT_B, BLOCK_B), (AT_C, BLOCK_C), (AT_D, BLOCK_D), (AT_E, BLOCK_E))

        lax.fori_loop(0, GROUP, send_far, 0)
        for some in (ways[0:2], ways[2:4], ways[4:5]):

            def send_own(j, _):
                to = (inner + j) % GROUP
                for at, block in some:
                    answer(at, first_group[block] + inner, block, z, to)
                return 0

            lax.fori_loop(1, GROUP, send_own, 0)
        for at, block in ways:
            returned[k, first_group[block] + inner] = product[k, at * GROUP + inner]

    def weighed(block, groups, k):
        remotes = groups - 1
        landed(returned.at[k, pl.ds(0, remotes)], ret_recv.at[block, k])
        rows = returned[k, pl.ds(first_group[block], groups)].reshape(groups * CAP, COL)
        lanes = slice(LANE[block], LANE[block] + groups * CAP)
        return jnp.dot(high[:, lanes], rows, preferred_element_type=F32) + jnp.dot(
            low[:, lanes], rows, preferred_element_type=F32
        )

    def send_partials(k):
        far[0, k] = weighed(BLOCK_A, 20, k).astype(BF16)
        remote(far.at[0, k], far_in.at[0, k], far_send, far_recv.at[0, k], down1, inner, tp).start()
        far[1, k] = weighed(BLOCK_B, 20, k).astype(BF16)
        remote(far.at[1, k], far_in.at[1, k], far_send, far_recv.at[1, k], up1, inner, tp).start()

    def add_partials(k):
        for side, block, to in ((0, BLOCK_C, down1), (1, BLOCK_D, up1)):
            here = weighed(block, 8, k)
            landed(far_in.at[side, k], far_recv.at[side, k])
            near[side, k] = (here + far_in[side, k].astype(F32)).astype(BF16)
            remote(near.at[side, k], near_in.at[side, k], near_send, near_recv.at[side, k], to, inner, tp).start()

    def close(k):
        n = columns_at(k)
        here = weighed(BLOCK_E, 8, k)
        landed(near_in.at[0, k], near_recv.at[0, k])
        landed(near_in.at[1, k], near_recv.at[1, k])
        t = tokens[:, pl.ds(pl.multiple_of(n * COL, COL), COL)].astype(F32)
        r = (t + here + near_in[0, k].astype(F32) + near_in[1, k].astype(F32)).astype(BF16)
        residual[k] = r
        s = r.astype(F32)
        s = s * s
        s = s[:, 0:128] + s[:, 128:256] + s[:, 256:384] + s[:, 384:512]
        squares[...] = s if k == 0 else squares[...] + s

        @pl.when(n != tp)
        def _():
            remote(residual.at[k], slices.at[tp], slice_send, slice_recv.at[tp], z, inner, n).start()

        @pl.when(n == tp)
        def _():
            slices[tp] = residual[k]

    contract(0)
    relay_down(1)
    contract(1)
    relay_down(2)
    send_partials(0)
    relay_down(3)
    contract(2)
    send_partials(1)
    add_partials(0)
    contract(3)
    send_partials(2)
    add_partials(1)
    close(0)
    send_partials(3)
    add_partials(2)
    close(1)
    add_partials(3)
    close(2)
    close(3)

    inverse = lax.rsqrt(jnp.sum(squares[...], axis=-1, keepdims=True) / D + EPS)
    inverse_out[...] = jnp.broadcast_to(inverse, (ROWS, 128)).T[0:8, :]
    lasts = [
        remote(inverse_out, inverses.at[tp], inv_send.at[k], inv_recv.at[k], z, inner, other)
        for k, other in enumerate((right, left, opposite))
    ]
    start(lasts)
    inverses[tp] = inverse_out[...]

    def finish(source):
        column = jnp.broadcast_to(inverses[source, 0:1, :], (128, ROWS)).T[:, 0:1]
        out[source] = (slices[source].astype(F32) * column * final_gain[...].astype(F32)[None, :]).astype(BF16)

    finish(tp)
    for copy in lasts:
        copy.wait_recv()
    for other in (right, left, opposite):
        landed(slices.at[other], slice_recv.at[other])
        finish(other)

    for copy in tells + flights + lasts + sum(outs, []) + sum(ons, []):
        copy.wait_send()
    sent(raw, raw_send)
    sent(routed.at[pl.ds(0, 59)], disp_send)
    sent(routed.at[pl.ds(0, 59)], ret_send)
    sent(far, far_send)
    sent(near, near_send)
    sent(slices.at[pl.ds(0, 3)], slice_send)


def local(
    tokens, norm_gain, expert_ids, group_weight, expert_logit, w_gate, w_up, w_down, final_gain
):
    vmem = pl.BlockSpec(memory_space=pltpu.VMEM)
    anywhere = pl.BlockSpec(memory_space=pl.ANY)
    dma, groups = pltpu.SemaphoreType.DMA, PLANES * GROUP
    out = pl.pallas_call(
        kernel,
        out_shape=jax.ShapeDtypeStruct((TP, ROWS, COL), BF16),
        in_specs=[vmem] * 5 + [anywhere] * 3 + [vmem],
        out_specs=vmem,
        scratch_shapes=[
            pltpu.VMEM((TP, ROWS, COL), BF16),
            pltpu.VMEM((4, TP, ROWS, COL), BF16),
            pltpu.VMEM((5, 8, ROWS), F32),
            pltpu.VMEM((groups * CAP, ROWS), BF16),
            pltpu.VMEM((groups, CAP, D), BF16),
            pltpu.VMEM((groups, CAP, D), BF16),
            pltpu.VMEM((TP, groups * CAP, FF // TP), BF16),
            pltpu.VMEM((TP, groups, CAP, COL), BF16),
            pltpu.VMEM((TP, groups, CAP, COL), BF16),
            pltpu.VMEM((TP, D, FF // TP), BF16),
            pltpu.VMEM((TP, D, FF // TP), BF16),
            pltpu.VMEM((TP, TP, FF // TP, COL), BF16),
            pltpu.VMEM((ROWS, 1152), BF16),
            pltpu.VMEM((ROWS, 1152), BF16),
            pltpu.VMEM((2, TP, ROWS, COL), BF16),
            pltpu.VMEM((2, TP, ROWS, COL), BF16),
            pltpu.VMEM((2, TP, ROWS, COL), BF16),
            pltpu.VMEM((2, TP, ROWS, COL), BF16),
            pltpu.VMEM((TP, ROWS, COL), BF16),
            pltpu.VMEM((TP, ROWS, COL), BF16),
            pltpu.VMEM((ROWS, 128), F32),
            pltpu.VMEM((8, ROWS), F32),
            pltpu.VMEM((TP, 8, ROWS), F32),
            dma((6,)), dma((6,)), dma((6,)), dma((TP, 6)), dma((TP, 6)), dma((4,)), dma((4,)), dma, dma((4, TP)),
            dma, dma((PLANES,)), dma, dma((5, TP)), dma, dma((2, TP)), dma, dma((2, TP)), dma, dma((TP,)),
            dma((3,)), dma((3,)),
        ],
        compiler_params=pltpu.CompilerParams(
            collective_id=0, has_side_effects=True, vmem_limit_bytes=62 * 1024 * 1024
        ),
    )(
        tokens, norm_gain, expert_ids.T, group_weight[None, :], expert_logit.T,
        w_gate[0], w_up[0], w_down[0], final_gain,
    )
    return out.reshape(TP * ROWS, COL)


def solution(mesh):
    placed = (
        P(("ep", "tp"), None),
        P(),
        P(("ep", "tp"), None),
        P(("ep", "tp")),
        P(("ep", "tp"), None),
        P("ep", None, "tp"),
        P("ep", None, "tp"),
        P("ep", "tp", None),
        P("tp"),
    )
    return jax.shard_map(
        local, mesh=mesh, in_specs=placed, out_specs=P("ep", "tp"), check_vma=False
    )
```

```python
import jax
import jax.numpy as jnp
from jax import lax
from jax.experimental import pallas as pl
from jax.experimental.pallas import tpu as pltpu
from jax.sharding import PartitionSpec as P

D = 2048
FF = 1024
CAP = 16
ROWS = 256
PLANES = 8
GROUP = 8
LANES = GROUP * CAP
TP = 4
COL = D // TP
HALF = COL // 2
STAGES = 2 * TP
EPS = 1e-06
MESH = pl.DeviceIdType.MESH
F32 = jnp.float32
BF16 = jnp.bfloat16

A, B, C, DD, E = 0, 20, 40, 48, 56
BLOCK_A, BLOCK_B, BLOCK_C, BLOCK_D, BLOCK_E = range(5)
AT_E, AT_C, AT_D, AT_A, AT_B, AT_UP, AT_DOWN, AT_FAR = range(8)
LANE = (0, 384, 768, 896, 1024)


def kernel(
    tokens_in, gain_in, ids_in, group_weight_in, logit_in, w_gate, w_up, w_down, final_gain_in, out,
    tokens, gain, ids, group_weight, logit, final_gain, done,
    normed, raw, info, pick, packed, routed, hidden, product, returned, wg, wu, wd, high, low,
    far, far_in, near, near_in, residual, slices, squares, inverse_out, inverses,
    in_sem, done_sem, own_sem, w_send, w_recv, d_send, d_recv, info_send, info_recv, raw_send, raw_recv, disp_send, disp_recv,
    ret_send, ret_recv, far_send, far_recv, near_send, near_recv, slice_send, slice_recv, inv_send, inv_recv,
):
    ep, tp = lax.axis_index("ep"), lax.axis_index("tp")
    z, inner = ep // GROUP, ep % GROUP
    up1, down1, up2, down2 = ((z + k) % PLANES for k in (1, 7, 2, 6))
    right, left, opposite = (tp + 1) % TP, (tp + 3) % TP, (tp + 2) % TP

    def remote(src, dst, send, recv, to_z, to_inner, to_tp):
        return pltpu.make_async_remote_copy(
            src_ref=src, dst_ref=dst, send_sem=send, recv_sem=recv,
            device_id={"ep": to_z * GROUP + to_inner, "tp": to_tp}, device_id_type=MESH,
        )

    def landed(dst, recv):
        remote(dst, dst, info_send.at[0], recv, z, inner, right).wait_recv()

    def sent(src, send):
        remote(src, src, send, info_recv.at[0], z, inner, right).wait_send()

    barrier = pltpu.get_barrier_semaphore()

    def greet(to_z, to_inner, to_tp):
        pl.semaphore_signal(
            barrier, inc=1, device_id={"ep": to_z * GROUP + to_inner, "tp": to_tp}, device_id_type=MESH
        )

    def greet_plane(i, _):
        o = i // GROUP
        greet((z + PLANES + (1 - 2 * (o % 2)) * (2 - o // 2)) % PLANES, i % GROUP, tp)
        return 0

    def greet_own(j, _):
        greet(z, (inner + j) % GROUP, tp)
        return 0

    lax.fori_loop(0, 4 * GROUP, greet_plane, 0)
    lax.fori_loop(1, GROUP, greet_own, 0)
    for other in (right, left, opposite):
        greet(z, inner, other)

    inputs = [
        pltpu.make_async_copy(src, dst, in_sem.at[k])
        for k, (src, dst) in enumerate((
            (tokens_in, tokens), (gain_in, gain), (ids_in, ids), (group_weight_in, group_weight),
            (logit_in, logit), (final_gain_in, final_gain),
        ))
    ]
    for copy in inputs:
        copy.start()
    own = [
        pltpu.make_async_copy(w_gate, wg.at[tp], own_sem.at[0]),
        pltpu.make_async_copy(w_up, wu.at[tp], own_sem.at[1]),
    ] + [
        pltpu.make_async_copy(w_down.at[:, pl.ds(n * COL, COL)], wd.at[tp, n], own_sem.at[2 + n]) for n in range(TP)
    ]
    for copy in inputs:
        copy.wait()
    for copy in own:
        copy.start()

    def norm_rows(i, _):
        at = pl.ds(pl.multiple_of(i * 32, 32), 32)
        t = tokens[at, :].astype(F32)
        inverse = lax.rsqrt(jnp.mean(t * t, axis=-1, keepdims=True) + EPS)
        t = (t * inverse * gain[...].astype(F32)[None, :]).astype(BF16)
        for n in range(TP):
            normed[n, at, :] = t[:, n * COL:(n + 1) * COL]
        return 0

    lax.fori_loop(0, ROWS // 32, norm_rows, 0)

    for copy in own:
        copy.wait()
    pl.semaphore_wait(barrier, 42)

    def weights(src, dst, k, to):
        copy = remote(src, dst, w_send.at[k], w_recv.at[k], z, inner, to)
        copy.start()
        return copy

    flights = [
        weights(wg.at[tp], wg.at[tp], 0, right),
        weights(wu.at[tp], wu.at[tp], 1, left),
        weights(wu.at[tp], wu.at[tp], 2, right),
        weights(wg.at[tp], wg.at[tp], 3, left),
    ]

    id0, id1 = ids[0:1, :], ids[1:2, :]
    lane = lax.broadcasted_iota(jnp.int32, (PLANES * GROUP, ROWS), 0)
    first, second = lane == id0, lane == id1
    named = jnp.where(first, 1.0, jnp.where(second, 1.0, 0.0)).astype(BF16)
    earlier = jnp.where(
        lax.broadcasted_iota(jnp.int32, (ROWS, ROWS), 0)
        < lax.broadcasted_iota(jnp.int32, (ROWS, ROWS), 1), 1.0, 0.0,
    ).astype(BF16)
    before = jnp.dot(named, earlier, preferred_element_type=F32)
    e0, e1 = jnp.exp(logit[0:1, :]), jnp.exp(logit[1:2, :])
    total = e0 + e1
    info[BLOCK_E, 0:1, :] = id0.astype(F32) * CAP + jnp.sum(jnp.where(first, before, 0.0), axis=0, keepdims=True)
    info[BLOCK_E, 1:2, :] = id1.astype(F32) * CAP + jnp.sum(jnp.where(second, before, 0.0), axis=0, keepdims=True)
    info[BLOCK_E, 2:3, :] = group_weight[...] * (e0 / total)
    info[BLOCK_E, 3:4, :] = group_weight[...] * (e1 / total)
    info[BLOCK_E, 4:8, :] = jnp.zeros((4, ROWS), F32)

    sections = {
        BLOCK_A: ((0, 128, z * LANES, 1), (128, 128, up1 * LANES, 1), (256, 64, up2 * LANES, 2)),
        BLOCK_B: ((0, 128, z * LANES, 1), (128, 128, down1 * LANES, 1), (256, 64, down2 * LANES + CAP, 2)),
        BLOCK_C: ((0, 128, z * LANES, 1),),
        BLOCK_D: ((0, 128, z * LANES, 1),),
        BLOCK_E: ((0, 128, z * LANES, 1),),
    }

    def slots(count, number, step):
        row = lax.broadcasted_iota(jnp.int32, (count, ROWS), 0)
        return (row + (step - 1) * CAP * lax.div(row, CAP) + number).astype(F32)

    first_group = {BLOCK_A: A, BLOCK_B: B, BLOCK_C: C, BLOCK_D: DD, BLOCK_E: E}

    def make_pick(block):
        at0, at1 = info[block, 0:1, :], info[block, 1:2, :]
        for start, count, number, step in sections[block]:
            slot = slots(count, number, step)
            row = first_group[block] * CAP + start
            pick[row:row + count, :] = jnp.where(slot == at0, 1.0, jnp.where(slot == at1, 1.0, 0.0)).astype(BF16)

    def make_weights(block):
        at0, at1, w0, w1 = (info[block, k:k + 1, :] for k in range(4))
        for start, count, number, step in sections[block]:
            slot = slots(128, number, step)
            w = (jnp.where(slot == at0, w0, 0.0) + jnp.where(slot == at1, w1, 0.0)).T[:, :count]
            top_term = w.astype(BF16)
            lanes = slice(LANE[block] + start, LANE[block] + start + count)
            high[:, lanes] = top_term
            low[:, lanes] = (w - top_term.astype(F32)).astype(BF16)

    def pack(block, groups, src, n):
        row = first_group[block] * CAP
        rows = jnp.dot(pick[row:row + groups * CAP, :], src, preferred_element_type=F32).astype(BF16)
        packed[pl.ds(first_group[block], groups), :, pl.ds(pl.multiple_of(n * COL, COL), COL)] = rows.reshape(
            groups, CAP, COL
        )

    def send_own_plane(ways, n):
        cols = pl.ds(pl.multiple_of(n * COL, COL), COL)

        def send(j, _):
            to = (inner + j) % GROUP
            for block, at in ways:
                remote(
                    packed.at[first_group[block] + to, :, cols], routed.at[at * GROUP + inner, :, cols], disp_send,
                    disp_recv.at[at], z, to, tp,
                ).start()
            return 0

        lax.fori_loop(1, GROUP, send, 0)
        for block, at in ways:
            routed[at * GROUP + inner, :, cols] = packed[first_group[block] + inner, :, cols]

    tells = [
        remote(info.at[BLOCK_E], info.at[block], info_send.at[block], info_recv.at[block], to, inner, tp)
        for block, to in ((BLOCK_C, up1), (BLOCK_D, down1), (BLOCK_A, up2), (BLOCK_B, down2))
    ]
    for copy in tells:
        copy.start()

    def hop_out(n, _):
        remote(normed.at[n], raw.at[0, n], raw_send, raw_recv.at[0, n], up1, inner, tp).start()
        remote(normed.at[n], raw.at[1, n], raw_send, raw_recv.at[1, n], down1, inner, tp).start()
        return 0

    lax.fori_loop(0, TP, hop_out, 0)

    make_pick(BLOCK_E)

    def pack_own(n, _):
        pack(BLOCK_E, 8, normed[n], n)
        send_own_plane(((BLOCK_E, AT_E),), n)
        return 0

    lax.fori_loop(0, TP, pack_own, 0)
    for copy in tells:
        copy.wait_recv()
    for block in (BLOCK_C, BLOCK_D, BLOCK_A, BLOCK_B):
        make_pick(block)

    def hop_on(n, _):
        landed(raw.at[0, n], raw_recv.at[0, n])
        remote(raw.at[0, n], raw.at[2, n], raw_send, raw_recv.at[2, n], up1, inner, tp).start()
        landed(raw.at[1, n], raw_recv.at[1, n])
        remote(raw.at[1, n], raw.at[3, n], raw_send, raw_recv.at[3, n], down1, inner, tp).start()
        pack(BLOCK_C, 8, raw[0, n], n)
        pack(BLOCK_D, 8, raw[1, n], n)
        send_own_plane(((BLOCK_C, AT_C), (BLOCK_D, AT_D)), n)
        return 0

    lax.fori_loop(0, TP, hop_on, 0)

    half = FF // TP // 2
    top, bottom = pl.ds(0, half), pl.ds(half, half)

    def over_y(q, n, part, k, to):
        return remote(wd.at[q, n, part], wd.at[q, n, part], d_send.at[n, k], d_recv.at[n, k], z, inner, to)

    def down_out(n):
        return [
            over_y(tp, n, top, 0, right), over_y(tp, n, bottom, 1, left),
            over_y(tp, n, bottom, 4, right), over_y(tp, n, top, 5, left),
        ]

    def down_on(n):
        return [over_y(left, n, top, 2, right), over_y(right, n, bottom, 3, left)]

    def start(copies):
        for copy in copies:
            copy.start()

    flights[0].wait_recv()
    flights.append(weights(wg.at[left], wg.at[left], 4, right))
    flights[1].wait_recv()
    flights.append(weights(wu.at[right], wu.at[right], 5, left))
    outs, ons = [down_out(n) for n in (0, 2, 3, 1)], [down_on(n) for n in (0, 2, 3, 1)]
    start(outs[0])

    def relay_down(k):
        outs[k][0].wait_recv()
        outs[k][1].wait_recv()
        start(ons[k])
        if k + 1 < TP:
            start(outs[k + 1])

    def expand(q, first_row, count):
        groups = count // CAP
        xs = routed[pl.ds(first_row // CAP, groups)].reshape(count, D)
        g = jnp.dot(xs, wg[q], preferred_element_type=F32)
        u = jnp.dot(xs, wu[q], preferred_element_type=F32)
        hidden[q, pl.ds(first_row, count), :] = (g / (1.0 + jnp.exp(-g)) * u).astype(BF16)

    def expand_of(order, first_row, count):
        def part(i, _):
            expand((tp + order[0] + order[1] * i) % TP, first_row, count)
            return 0

        lax.fori_loop(0, order[2], part, 0)

    def rows_landed(at, groups):
        landed(routed.at[pl.ds(0, groups)], disp_recv.at[at])

    for block in range(5):
        make_weights(block)
    rows_landed(AT_E, GROUP - 1)
    rows_landed(AT_C, GROUP - 1)
    rows_landed(AT_D, GROUP - 1)
    expand_of((0, 0, 1), 0, 384)

    def hop_last(n, _):
        landed(raw.at[2, n], raw_recv.at[2, n])
        landed(raw.at[3, n], raw_recv.at[3, n])
        pack(BLOCK_A, 20, raw[2, n], n)
        pack(BLOCK_B, 20, raw[3, n], n)
        send_own_plane(((BLOCK_A, AT_A), (BLOCK_B, AT_B)), n)
        cols = pl.ds(pl.multiple_of(n * COL, COL), COL)

        def send_next(i, _):
            remote(
                packed.at[A + 8 + i, :, cols], routed.at[AT_UP * GROUP + inner, :, cols], disp_send,
                disp_recv.at[AT_UP], up1, i, tp,
            ).start()
            remote(
                packed.at[B + 8 + i, :, cols], routed.at[AT_DOWN * GROUP + inner, :, cols], disp_send,
                disp_recv.at[AT_DOWN], down1, i, tp,
            ).start()
            return 0

        def send_far(i, _):
            remote(
                packed.at[A + 16 + i, :, cols], routed.at[AT_FAR * GROUP + inner, :, cols], disp_send,
                disp_recv.at[AT_FAR], up2, 2 * i, tp,
            ).start()
            remote(
                packed.at[B + 16 + i, :, cols], routed.at[AT_FAR * GROUP + inner, :, cols], disp_send,
                disp_recv.at[AT_FAR], down2, 2 * i + 1, tp,
            ).start()
            return 0

        lax.fori_loop(0, 4, send_far, 0)
        lax.fori_loop(0, GROUP, send_next, 0)
        return 0

    lax.fori_loop(0, TP, hop_last, 0)

    flights[2].wait_recv()
    flights[3].wait_recv()
    expand_of((1, 2, 2), 0, 384)
    rows_landed(AT_A, GROUP - 1)
    rows_landed(AT_B, GROUP - 1)
    expand_of((3, 1, 3), 384, 256)
    flights[4].wait_recv()
    flights[5].wait_recv()
    expand_of((2, 0, 1), 0, 640)
    relay_down(0)
    rows_landed(AT_UP, GROUP)
    rows_landed(AT_DOWN, GROUP)
    rows_landed(AT_FAR, GROUP)
    expand_of((0, 1, 4), 640, 384)

    last = tp // 3

    def columns_at(k):
        if k < 5:
            return (0, 0, 2, 2, 3)[k], k % 2
        return (3 - 2 * last, 1, 1 + 2 * last)[k - 5], (1 - last, last, 1)[k - 5]

    odd = inner % 2
    ways = ((AT_A, BLOCK_A), (AT_B, BLOCK_B), (AT_C, BLOCK_C), (AT_D, BLOCK_D), (AT_E, BLOCK_E))

    def contract(k):
        n, h = columns_at(k)
        cols = pl.ds(pl.multiple_of(h * HALF, HALF), HALF)
        if k in (0, 2, 4, 5):
            for sem in range(2, 6):
                landed(wd.at[opposite, 0, top], d_recv.at[(0, 0, 2, 2, 3, 1)[k], sem])

        def part(i, _):
            at = pl.ds(pl.multiple_of(i * 256, 256), 256)
            rows = jnp.dot(hidden[0, at, :], wd[0, n, :, cols], preferred_element_type=F32)
            for q in range(1, TP):
                rows += jnp.dot(hidden[q, at, :], wd[q, n, :, cols], preferred_element_type=F32)
            product[k, pl.ds(i * 16, 16)] = rows.astype(BF16).reshape(16, CAP, HALF)
            return 0

        lax.fori_loop(0, 4, part, 0)

        def send_far(i, _):
            answer(k, AT_FAR, A + 16 + inner // 2 + (B - A) * odd, odd, (z + 6 + 4 * odd) % PLANES, i)
            answer(k, AT_UP, A + 8 + inner, BLOCK_A, down1, i)
            answer(k, AT_DOWN, B + 8 + inner, BLOCK_B, up1, i)
            return 0

        lax.fori_loop(0, GROUP, send_far, 0)
        answer_plane(k, ways[0:2])

    def answer(k, at, group, block, to_z, i):
        remote(product.at[k, at * GROUP + i], returned.at[k, group], ret_send, ret_recv.at[block, k], to_z, i, tp).start()

    def answer_plane(k, some):
        def send_own(j, _):
            to = (inner + j) % GROUP
            for at, block in some:
                answer(k, at, first_group[block] + inner, block, z, to)
            return 0

        lax.fori_loop(1, GROUP, send_own, 0)
        for at, block in some:
            returned[k, first_group[block] + inner] = product[k, at * GROUP + inner]

    def answer_near(k):
        answer_plane(k, ways[2:4])
        answer_plane(k, ways[4:5])

    def weighed(block, groups, k):
        remotes = groups - 1
        landed(returned.at[k, pl.ds(0, remotes)], ret_recv.at[block, k])
        rows = returned[k, pl.ds(first_group[block], groups)].reshape(groups * CAP, HALF)
        lanes = slice(LANE[block], LANE[block] + groups * CAP)
        return jnp.dot(high[:, lanes], rows, preferred_element_type=F32) + jnp.dot(
            low[:, lanes], rows, preferred_element_type=F32
        )

    def send_partials(k):
        far[0, k] = weighed(BLOCK_A, 20, k).astype(BF16)
        remote(far.at[0, k], far_in.at[0, k], far_send, far_recv.at[0, k], down1, inner, tp).start()
        far[1, k] = weighed(BLOCK_B, 20, k).astype(BF16)
        remote(far.at[1, k], far_in.at[1, k], far_send, far_recv.at[1, k], up1, inner, tp).start()

    def add_partials(k):
        for side, block, to in ((0, BLOCK_C, down1), (1, BLOCK_D, up1)):
            here = weighed(block, 8, k)
            landed(far_in.at[side, k], far_recv.at[side, k])
            near[side, k] = (here + far_in[side, k].astype(F32)).astype(BF16)
            remote(near.at[side, k], near_in.at[side, k], near_send, near_recv.at[side, k], to, inner, tp).start()

    def close(k):
        n, h = columns_at(k)
        here = weighed(BLOCK_E, 8, k)
        landed(near_in.at[0, k], near_recv.at[0, k])
        landed(near_in.at[1, k], near_recv.at[1, k])
        t = tokens[:, pl.ds(pl.multiple_of(n * COL + h * HALF, HALF), HALF)].astype(F32)
        r = (t + here + near_in[0, k].astype(F32) + near_in[1, k].astype(F32)).astype(BF16)
        residual[k] = r
        s = r.astype(F32)
        s = s * s
        s = s[:, 0:128] + s[:, 128:256]
        squares[...] = s if k == 0 else squares[...] + s

        @pl.when(n != tp)
        def _():
            remote(residual.at[k], slices.at[tp, h], slice_send, slice_recv.at[tp], z, inner, n).start()

        @pl.when(n == tp)
        def _():
            slices[tp, h] = residual[k]

    contract(0)
    contract(1)
    answer_near(0)
    relay_down(1)
    answer_near(1)
    send_partials(0)
    contract(2)
    send_partials(1)
    answer_near(2)
    relay_down(2)
    contract(3)
    answer_near(3)
    add_partials(0)
    send_partials(2)
    add_partials(1)
    relay_down(3)
    close(0)
    contract(4)
    answer_near(4)
    send_partials(3)
    add_partials(2)
    close(1)
    contract(5)
    answer_near(5)
    send_partials(4)
    add_partials(3)
    close(2)
    contract(6)
    answer_near(6)
    send_partials(5)
    add_partials(4)
    close(3)
    contract(7)
    answer_near(7)
    send_partials(6)
    add_partials(5)
    close(4)
    send_partials(7)
    add_partials(6)
    close(5)
    add_partials(7)
    close(6)
    close(7)

    inverse = lax.rsqrt(jnp.sum(squares[...], axis=-1, keepdims=True) / D + EPS)
    inverse_out[...] = jnp.broadcast_to(inverse, (ROWS, 128)).T[0:8, :]
    lasts = [
        remote(inverse_out, inverses.at[tp], inv_send.at[k], inv_recv.at[k], z, inner, other)
        for k, other in enumerate((right, left, opposite))
    ]
    start(lasts)
    inverses[tp] = inverse_out[...]

    def finish(source):
        column = jnp.broadcast_to(inverses[source, 0:1, :], (128, ROWS)).T[:, 0:1]
        for h in range(2):
            cols = slice(h * HALF, (h + 1) * HALF)
            t = slices[source, h].astype(F32) * column * final_gain[cols].astype(F32)[None, :]
            done[source, :, cols] = t.astype(BF16)

    finish(tp)
    for copy, other in zip(lasts, (left, right, opposite)):
        copy.wait_recv()
        landed(slices.at[other], slice_recv.at[other])
        finish(other)
    results = [pltpu.make_async_copy(done.at[n], out.at[n], done_sem.at[n]) for n in range(TP)]
    start(results)

    for copy in tells + flights + lasts + sum(outs, []) + sum(ons, []):
        copy.wait_send()
    for copy in results:
        copy.wait()
    sent(raw, raw_send)
    sent(routed.at[pl.ds(0, 59)], disp_send)
    sent(routed.at[pl.ds(0, 59)], ret_send)
    sent(far, far_send)
    sent(near, near_send)
    sent(slices.at[pl.ds(0, 3)], slice_send)


def local(
    tokens, norm_gain, expert_ids, group_weight, expert_logit, w_gate, w_up, w_down, final_gain
):
    anywhere = pl.BlockSpec(memory_space=pl.ANY)
    dma, groups = pltpu.SemaphoreType.DMA, PLANES * GROUP
    out = pl.pallas_call(
        kernel,
        out_shape=jax.ShapeDtypeStruct((TP, ROWS, COL), BF16),
        in_specs=[anywhere] * 9,
        out_specs=anywhere,
        scratch_shapes=[
            pltpu.VMEM((ROWS, D), BF16),
            pltpu.VMEM((D,), BF16),
            pltpu.VMEM((2, ROWS), jnp.int32),
            pltpu.VMEM((1, ROWS), F32),
            pltpu.VMEM((2, ROWS), F32),
            pltpu.VMEM((COL,), BF16),
            pltpu.VMEM((TP, ROWS, COL), BF16),
            pltpu.VMEM((TP, ROWS, COL), BF16),
            pltpu.VMEM((4, TP, ROWS, COL), BF16),
            pltpu.VMEM((5, 8, ROWS), F32),
            pltpu.VMEM((groups * CAP, ROWS), BF16),
            pltpu.VMEM((groups, CAP, D), BF16),
            pltpu.VMEM((groups, CAP, D), BF16),
            pltpu.VMEM((TP, groups * CAP, FF // TP), BF16),
            pltpu.VMEM((STAGES, groups, CAP, HALF), BF16),
            pltpu.VMEM((STAGES, groups, CAP, HALF), BF16),
            pltpu.VMEM((TP, D, FF // TP), BF16),
            pltpu.VMEM((TP, D, FF // TP), BF16),
            pltpu.VMEM((TP, TP, FF // TP, COL), BF16),
            pltpu.VMEM((ROWS, 1152), BF16),
            pltpu.VMEM((ROWS, 1152), BF16),
            pltpu.VMEM((2, STAGES, ROWS, HALF), BF16),
            pltpu.VMEM((2, STAGES, ROWS, HALF), BF16),
            pltpu.VMEM((2, STAGES, ROWS, HALF), BF16),
            pltpu.VMEM((2, STAGES, ROWS, HALF), BF16),
            pltpu.VMEM((STAGES, ROWS, HALF), BF16),
            pltpu.VMEM((TP, 2, ROWS, HALF), BF16),
            pltpu.VMEM((ROWS, 128), F32),
            pltpu.VMEM((8, ROWS), F32),
            pltpu.VMEM((TP, 8, ROWS), F32),
            dma((6,)), dma((TP,)), dma((6,)), dma((6,)), dma((6,)), dma((TP, 6)), dma((TP, 6)), dma((4,)), dma((4,)), dma, dma((4, TP)),
            dma, dma((PLANES,)), dma, dma((5, STAGES)), dma, dma((2, STAGES)), dma, dma((2, STAGES)), dma, dma((TP,)),
            dma((3,)), dma((3,)),
        ],
        compiler_params=pltpu.CompilerParams(
            collective_id=0, has_side_effects=True, vmem_limit_bytes=62 * 1024 * 1024
        ),
    )(
        tokens, norm_gain, expert_ids.T, group_weight[None, :], expert_logit.T,
        w_gate[0], w_up[0], w_down[0], final_gain,
    )
    return out.reshape(TP * ROWS, COL)


def solution(mesh):
    placed = (
        P(("ep", "tp"), None),
        P(),
        P(("ep", "tp"), None),
        P(("ep", "tp")),
        P(("ep", "tp"), None),
        P("ep", None, "tp"),
        P("ep", None, "tp"),
        P("ep", "tp", None),
        P("tp"),
    )
    return jax.shard_map(
        local, mesh=mesh, in_specs=placed, out_specs=P("ep", "tp"), check_vma=False
    )
```

```python
import jax
import jax.numpy as jnp
from jax import lax
from jax.experimental import pallas as pl
from jax.experimental.pallas import tpu as pltpu
from jax.sharding import PartitionSpec as P

D = 2048
FF = 1024
CAP = 16
ROWS = 256
PLANES = 8
GROUP = 8
LANES = GROUP * CAP
TP = 4
COL = D // TP
HALF = COL // 2
STAGES = 2 * TP
EPS = 1e-06
MESH = pl.DeviceIdType.MESH
F32 = jnp.float32
BF16 = jnp.bfloat16

A, B, C, DD, E = 0, 20, 40, 48, 56
BLOCK_A, BLOCK_B, BLOCK_C, BLOCK_D, BLOCK_E = range(5)
AT_E, AT_C, AT_D, AT_A, AT_B, AT_UP, AT_DOWN, AT_FAR = range(8)
LANE = (0, 384, 768, 896, 1024)


def kernel(
    tokens_in, gain_in, ids_in, group_weight_in, logit_in, w_gate, w_up, w_down, final_gain_in, out,
    tokens, gain, ids, group_weight, logit, final_gain,
    normed, raw, info, pick, packed, routed, hidden, product, returned, wg, wu, wd, high, low,
    far, far_in, near, near_in, residual, slices, squares, inverse_out, inverses,
    in_sem, own_sem, w_send, w_recv, d_send, d_recv, info_send, info_recv, raw_send, raw_recv, disp_send, disp_recv,
    ret_send, ret_recv, far_send, far_recv, near_send, near_recv, slice_send, slice_recv, inv_send, inv_recv,
):
    ep, tp = lax.axis_index("ep"), lax.axis_index("tp")
    z, inner = ep // GROUP, ep % GROUP
    up1, down1, up2, down2 = ((z + k) % PLANES for k in (1, 7, 2, 6))
    right, left, opposite = (tp + 1) % TP, (tp + 3) % TP, (tp + 2) % TP

    def remote(src, dst, send, recv, to_z, to_inner, to_tp):
        return pltpu.make_async_remote_copy(
            src_ref=src, dst_ref=dst, send_sem=send, recv_sem=recv,
            device_id={"ep": to_z * GROUP + to_inner, "tp": to_tp}, device_id_type=MESH,
        )

    def landed(dst, recv):
        remote(dst, dst, info_send.at[0], recv, z, inner, right).wait_recv()

    def sent(src, send):
        remote(src, src, send, info_recv.at[0], z, inner, right).wait_send()

    barrier = pltpu.get_barrier_semaphore()

    def greet(to_z, to_inner, to_tp):
        pl.semaphore_signal(
            barrier, inc=1, device_id={"ep": to_z * GROUP + to_inner, "tp": to_tp}, device_id_type=MESH
        )

    def greet_plane(i, _):
        o = i // GROUP
        greet((z + PLANES + (1 - 2 * (o % 2)) * (2 - o // 2)) % PLANES, i % GROUP, tp)
        return 0

    def greet_own(j, _):
        greet(z, (inner + j) % GROUP, tp)
        return 0

    lax.fori_loop(0, 4 * GROUP, greet_plane, 0)
    lax.fori_loop(1, GROUP, greet_own, 0)
    for other in (right, left, opposite):
        greet(z, inner, other)

    inputs = [
        pltpu.make_async_copy(src, dst, in_sem.at[k])
        for k, (src, dst) in enumerate((
            (tokens_in, tokens), (gain_in, gain), (ids_in, ids), (group_weight_in, group_weight),
            (logit_in, logit), (final_gain_in, final_gain),
        ))
    ]
    for copy in inputs:
        copy.start()
    own = [
        pltpu.make_async_copy(w_gate, wg.at[tp], own_sem.at[0]),
        pltpu.make_async_copy(w_up, wu.at[tp], own_sem.at[1]),
    ] + [
        pltpu.make_async_copy(w_down.at[:, pl.ds(n * COL, COL)], wd.at[tp, n], own_sem.at[2 + n]) for n in range(TP)
    ]
    for copy in inputs:
        copy.wait()
    for copy in own:
        copy.start()

    def norm_rows(i, _):
        at = pl.ds(pl.multiple_of(i * 32, 32), 32)
        t = tokens[at, :].astype(F32)
        inverse = lax.rsqrt(jnp.mean(t * t, axis=-1, keepdims=True) + EPS)
        t = (t * inverse * gain[...].astype(F32)[None, :]).astype(BF16)
        for n in range(TP):
            normed[n, at, :] = t[:, n * COL:(n + 1) * COL]
        return 0

    lax.fori_loop(0, ROWS // 32, norm_rows, 0)

    for copy in own:
        copy.wait()
    pl.semaphore_wait(barrier, 42)

    def weights(src, dst, k, to):
        copy = remote(src, dst, w_send.at[k], w_recv.at[k], z, inner, to)
        copy.start()
        return copy

    flights = [
        weights(wg.at[tp], wg.at[tp], 0, right),
        weights(wu.at[tp], wu.at[tp], 1, left),
        weights(wu.at[tp], wu.at[tp], 2, right),
        weights(wg.at[tp], wg.at[tp], 3, left),
    ]

    id0, id1 = ids[0:1, :], ids[1:2, :]
    lane = lax.broadcasted_iota(jnp.int32, (PLANES * GROUP, ROWS), 0)
    first, second = lane == id0, lane == id1
    named = jnp.where(first, 1.0, jnp.where(second, 1.0, 0.0)).astype(BF16)
    earlier = jnp.where(
        lax.broadcasted_iota(jnp.int32, (ROWS, ROWS), 0)
        < lax.broadcasted_iota(jnp.int32, (ROWS, ROWS), 1), 1.0, 0.0,
    ).astype(BF16)
    before = jnp.dot(named, earlier, preferred_element_type=F32)
    e0, e1 = jnp.exp(logit[0:1, :]), jnp.exp(logit[1:2, :])
    total = e0 + e1
    info[BLOCK_E, 0:1, :] = id0.astype(F32) * CAP + jnp.sum(jnp.where(first, before, 0.0), axis=0, keepdims=True)
    info[BLOCK_E, 1:2, :] = id1.astype(F32) * CAP + jnp.sum(jnp.where(second, before, 0.0), axis=0, keepdims=True)
    info[BLOCK_E, 2:3, :] = group_weight[...] * (e0 / total)
    info[BLOCK_E, 3:4, :] = group_weight[...] * (e1 / total)
    info[BLOCK_E, 4:8, :] = jnp.zeros((4, ROWS), F32)

    sections = {
        BLOCK_A: ((0, 128, z * LANES, 1), (128, 128, up1 * LANES, 1), (256, 64, up2 * LANES, 2)),
        BLOCK_B: ((0, 128, z * LANES, 1), (128, 128, down1 * LANES, 1), (256, 64, down2 * LANES + CAP, 2)),
        BLOCK_C: ((0, 128, z * LANES, 1),),
        BLOCK_D: ((0, 128, z * LANES, 1),),
        BLOCK_E: ((0, 128, z * LANES, 1),),
    }

    def slots(count, number, step):
        row = lax.broadcasted_iota(jnp.int32, (count, ROWS), 0)
        return (row + (step - 1) * CAP * lax.div(row, CAP) + number).astype(F32)

    first_group = {BLOCK_A: A, BLOCK_B: B, BLOCK_C: C, BLOCK_D: DD, BLOCK_E: E}

    def make_pick(block):
        at0, at1 = info[block, 0:1, :], info[block, 1:2, :]
        for start, count, number, step in sections[block]:
            slot = slots(count, number, step)
            row = first_group[block] * CAP + start
            pick[row:row + count, :] = jnp.where(slot == at0, 1.0, jnp.where(slot == at1, 1.0, 0.0)).astype(BF16)

    def make_weights(block):
        at0, at1, w0, w1 = (info[block, k:k + 1, :] for k in range(4))
        for start, count, number, step in sections[block]:
            slot = slots(128, number, step)
            w = (jnp.where(slot == at0, w0, 0.0) + jnp.where(slot == at1, w1, 0.0)).T[:, :count]
            top_term = w.astype(BF16)
            lanes = slice(LANE[block] + start, LANE[block] + start + count)
            high[:, lanes] = top_term
            low[:, lanes] = (w - top_term.astype(F32)).astype(BF16)

    def pack(block, groups, src, n):
        row = first_group[block] * CAP
        rows = jnp.dot(pick[row:row + groups * CAP, :], src, preferred_element_type=F32).astype(BF16)
        packed[pl.ds(first_group[block], groups), :, pl.ds(pl.multiple_of(n * COL, COL), COL)] = rows.reshape(
            groups, CAP, COL
        )

    def send_own_plane(ways, n):
        cols = pl.ds(pl.multiple_of(n * COL, COL), COL)

        def send(j, _):
            to = (inner + j) % GROUP
            for block, at in ways:
                remote(
                    packed.at[first_group[block] + to, :, cols], routed.at[at * GROUP + inner, :, cols], disp_send,
                    disp_recv.at[at], z, to, tp,
                ).start()
            return 0

        lax.fori_loop(1, GROUP, send, 0)
        for block, at in ways:
            routed[at * GROUP + inner, :, cols] = packed[first_group[block] + inner, :, cols]

    tells = [
        remote(info.at[BLOCK_E], info.at[block], info_send.at[block], info_recv.at[block], to, inner, tp)
        for block, to in ((BLOCK_C, up1), (BLOCK_D, down1), (BLOCK_A, up2), (BLOCK_B, down2))
    ]
    for copy in tells:
        copy.start()

    def hop_out(n, _):
        remote(normed.at[n], raw.at[0, n], raw_send, raw_recv.at[0, n], up1, inner, tp).start()
        remote(normed.at[n], raw.at[1, n], raw_send, raw_recv.at[1, n], down1, inner, tp).start()
        return 0

    lax.fori_loop(0, TP, hop_out, 0)

    make_pick(BLOCK_E)

    def pack_own(n, _):
        pack(BLOCK_E, 8, normed[n], n)
        send_own_plane(((BLOCK_E, AT_E),), n)
        return 0

    lax.fori_loop(0, TP, pack_own, 0)
    for copy in tells:
        copy.wait_recv()
    for block in (BLOCK_C, BLOCK_D, BLOCK_A, BLOCK_B):
        make_pick(block)

    def hop_on(n, _):
        landed(raw.at[0, n], raw_recv.at[0, n])
        remote(raw.at[0, n], raw.at[2, n], raw_send, raw_recv.at[2, n], up1, inner, tp).start()
        landed(raw.at[1, n], raw_recv.at[1, n])
        remote(raw.at[1, n], raw.at[3, n], raw_send, raw_recv.at[3, n], down1, inner, tp).start()
        pack(BLOCK_C, 8, raw[0, n], n)
        pack(BLOCK_D, 8, raw[1, n], n)
        send_own_plane(((BLOCK_C, AT_C), (BLOCK_D, AT_D)), n)
        return 0

    lax.fori_loop(0, TP, hop_on, 0)

    half = FF // TP // 2
    top, bottom = pl.ds(0, half), pl.ds(half, half)

    def over_y(q, piece, part, k, to):
        block = wd.at[q, piece % TP, part, pl.ds(piece // TP * HALF, HALF)]
        return remote(block, block, d_send.at[piece, k], d_recv.at[piece, k], z, inner, to)

    def down_out(piece):
        return [
            over_y(tp, piece, top, 0, right), over_y(tp, piece, bottom, 1, left),
            over_y(tp, piece, bottom, 4, right), over_y(tp, piece, top, 5, left),
        ]

    def down_on(piece):
        return [over_y(left, piece, top, 2, right), over_y(right, piece, bottom, 3, left)]

    def start(copies):
        for copy in copies:
            copy.start()

    flights[0].wait_recv()
    flights.append(weights(wg.at[left], wg.at[left], 4, right))
    flights[1].wait_recv()
    flights.append(weights(wu.at[right], wu.at[right], 5, left))
    outs, ons = [down_out(k) for k in range(STAGES)], [down_on(k) for k in range(STAGES)]
    start(outs[0])

    def relay_down(k):
        outs[k][0].wait_recv()
        outs[k][1].wait_recv()
        start(ons[k])
        for later in ((1,), (2,), (3, 4), (5,), (6,), (7,), (), ())[k]:
            start(outs[later])

    def expand(q, first_row, count):
        groups = count // CAP
        xs = routed[pl.ds(first_row // CAP, groups)].reshape(count, D)
        g = jnp.dot(xs, wg[q], preferred_element_type=F32)
        u = jnp.dot(xs, wu[q], preferred_element_type=F32)
        hidden[q, pl.ds(first_row, count), :] = (g / (1.0 + jnp.exp(-g)) * u).astype(BF16)

    def expand_of(order, first_row, count):
        def part(i, _):
            expand((tp + order[0] + order[1] * i) % TP, first_row, count)
            return 0

        lax.fori_loop(0, order[2], part, 0)

    def rows_landed(at, groups):
        landed(routed.at[pl.ds(0, groups)], disp_recv.at[at])

    for block in range(5):
        make_weights(block)
    rows_landed(AT_E, GROUP - 1)
    rows_landed(AT_C, GROUP - 1)
    rows_landed(AT_D, GROUP - 1)
    expand_of((0, 0, 1), 0, 384)

    def hop_last(n, _):
        landed(raw.at[2, n], raw_recv.at[2, n])
        landed(raw.at[3, n], raw_recv.at[3, n])
        pack(BLOCK_A, 20, raw[2, n], n)
        pack(BLOCK_B, 20, raw[3, n], n)
        send_own_plane(((BLOCK_A, AT_A), (BLOCK_B, AT_B)), n)
        cols = pl.ds(pl.multiple_of(n * COL, COL), COL)

        def send_next(i, _):
            remote(
                packed.at[A + 8 + i, :, cols], routed.at[AT_UP * GROUP + inner, :, cols], disp_send,
                disp_recv.at[AT_UP], up1, i, tp,
            ).start()
            remote(
                packed.at[B + 8 + i, :, cols], routed.at[AT_DOWN * GROUP + inner, :, cols], disp_send,
                disp_recv.at[AT_DOWN], down1, i, tp,
            ).start()
            return 0

        def send_far(i, _):
            remote(
                packed.at[A + 16 + i, :, cols], routed.at[AT_FAR * GROUP + inner, :, cols], disp_send,
                disp_recv.at[AT_FAR], up2, 2 * i, tp,
            ).start()
            remote(
                packed.at[B + 16 + i, :, cols], routed.at[AT_FAR * GROUP + inner, :, cols], disp_send,
                disp_recv.at[AT_FAR], down2, 2 * i + 1, tp,
            ).start()
            return 0

        lax.fori_loop(0, 4, send_far, 0)
        lax.fori_loop(0, GROUP, send_next, 0)
        return 0

    lax.fori_loop(0, TP, hop_last, 0)

    flights[2].wait_recv()
    flights[3].wait_recv()
    expand_of((1, 2, 2), 0, 384)
    rows_landed(AT_A, GROUP - 1)
    rows_landed(AT_B, GROUP - 1)
    expand_of((3, 1, 3), 384, 256)
    flights[4].wait_recv()
    flights[5].wait_recv()
    expand_of((2, 0, 1), 0, 640)
    relay_down(0)
    rows_landed(AT_UP, GROUP)
    rows_landed(AT_DOWN, GROUP)
    rows_landed(AT_FAR, GROUP)
    expand_of((0, 1, 4), 640, 384)

    def columns_at(k):
        if k < TP:
            return k, 0
        if k < STAGES - 1:
            return k - TP + (k - tp) // TP, 1
        return tp, 1

    odd = inner % 2
    ways = ((AT_A, BLOCK_A), (AT_B, BLOCK_B), (AT_C, BLOCK_C), (AT_D, BLOCK_D), (AT_E, BLOCK_E))

    def contract(k):
        n, h = columns_at(k)
        cols = pl.ds(h * HALF, HALF)
        for piece in ((0,), (1,), (2,), (3,), (4, 5), (6,), (7,), ())[k]:
            for copy in outs[piece][2:] + ons[piece]:
                copy.wait_recv()

        def part(i, _):
            i = 3 - i
            at = pl.ds(pl.multiple_of(i * 256, 256), 256)
            rows = jnp.dot(hidden[0, at, :], wd[0, n, :, cols], preferred_element_type=F32)
            for q in range(1, TP):
                rows += jnp.dot(hidden[q, at, :], wd[q, n, :, cols], preferred_element_type=F32)
            product[k, pl.ds(i * 16, 16)] = rows.astype(BF16).reshape(16, CAP, HALF)
            return 0

        lax.fori_loop(0, 2, part, 0)

        def send_far(i, _):
            answer(k, AT_FAR, A + 16 + inner // 2 + (B - A) * odd, odd, (z + 6 + 4 * odd) % PLANES, i)
            answer(k, AT_UP, A + 8 + inner, BLOCK_A, down1, i)
            answer(k, AT_DOWN, B + 8 + inner, BLOCK_B, up1, i)
            return 0

        lax.fori_loop(0, GROUP, send_far, 0)
        lax.fori_loop(2, 4, part, 0)
        answer_plane(k, ways[0:2])

    def answer(k, at, group, block, to_z, i):
        remote(product.at[k, at * GROUP + i], returned.at[k, group], ret_send, ret_recv.at[block, k], to_z, i, tp).start()

    def answer_plane(k, some):
        def send_own(j, _):
            to = (inner + j) % GROUP
            for at, block in some:
                answer(k, at, first_group[block] + inner, block, z, to)
            return 0

        lax.fori_loop(1, GROUP, send_own, 0)
        for at, block in some:
            returned[k, first_group[block] + inner] = product[k, at * GROUP + inner]

    def answer_near(k):
        answer_plane(k, ways[2:4])
        answer_plane(k, ways[4:5])

    def weighed(block, groups, k):
        remotes = groups - 1
        landed(returned.at[k, pl.ds(0, remotes)], ret_recv.at[block, k])
        rows = returned[k, pl.ds(first_group[block], groups)].reshape(groups * CAP, HALF)
        lanes = slice(LANE[block], LANE[block] + groups * CAP)
        return jnp.dot(high[:, lanes], rows, preferred_element_type=F32) + jnp.dot(
            low[:, lanes], rows, preferred_element_type=F32
        )

    def send_partials(k):
        far[0, k] = weighed(BLOCK_A, 20, k).astype(BF16)
        remote(far.at[0, k], far_in.at[0, k], far_send, far_recv.at[0, k], down1, inner, tp).start()
        far[1, k] = weighed(BLOCK_B, 20, k).astype(BF16)
        remote(far.at[1, k], far_in.at[1, k], far_send, far_recv.at[1, k], up1, inner, tp).start()

    def add_partials(k):
        for side, block, to in ((0, BLOCK_C, down1), (1, BLOCK_D, up1)):
            here = weighed(block, 8, k)
            landed(far_in.at[side, k], far_recv.at[side, k])
            near[side, k] = (here + far_in[side, k].astype(F32)).astype(BF16)
            remote(near.at[side, k], near_in.at[side, k], near_send, near_recv.at[side, k], to, inner, tp).start()

    def close(k):
        n, h = columns_at(k)
        here = weighed(BLOCK_E, 8, k)
        landed(near_in.at[0, k], near_recv.at[0, k])
        landed(near_in.at[1, k], near_recv.at[1, k])
        t = tokens[:, pl.ds(pl.multiple_of(n * COL + h * HALF, HALF), HALF)].astype(F32)
        r = (t + here + near_in[0, k].astype(F32) + near_in[1, k].astype(F32)).astype(BF16)
        residual[k] = r
        s = r.astype(F32)
        s = s * s
        s = s[:, 0:128] + s[:, 128:256]
        squares[...] = s if k == 0 else squares[...] + s

        @pl.when(n != tp)
        def _():
            remote(residual.at[k], slices.at[tp, h], slice_send, slice_recv.at[tp], z, inner, n).start()

        @pl.when(n == tp)
        def _():
            slices[tp, h] = residual[k]

    relay_down(1)
    contract(0)
    contract(1)
    answer_near(0)
    relay_down(2)
    answer_near(1)
    send_partials(0)
    contract(2)
    relay_down(3)
    send_partials(1)
    answer_near(2)
    contract(3)
    relay_down(4)
    answer_near(3)
    add_partials(0)
    send_partials(2)
    relay_down(5)
    add_partials(1)
    relay_down(6)
    close(0)
    contract(4)
    relay_down(7)
    answer_near(4)
    send_partials(3)
    add_partials(2)
    close(1)
    contract(5)
    answer_near(5)
    send_partials(4)
    add_partials(3)
    close(2)
    contract(6)
    answer_near(6)
    send_partials(5)
    add_partials(4)
    close(3)
    contract(7)
    answer_near(7)
    send_partials(6)
    add_partials(5)
    close(4)
    send_partials(7)
    add_partials(6)
    close(5)
    add_partials(7)
    close(6)
    close(7)

    inverse = lax.rsqrt(jnp.sum(squares[...], axis=-1, keepdims=True) / D + EPS)
    inverse_out[...] = jnp.broadcast_to(inverse, (ROWS, 128)).T[0:8, :]
    lasts = [
        remote(inverse_out, inverses.at[tp], inv_send.at[k], inv_recv.at[k], z, inner, other)
        for k, other in enumerate((right, left, opposite))
    ]
    start(lasts)
    inverses[tp] = inverse_out[...]

    def finish(source):
        column = jnp.broadcast_to(inverses[source, 0:1, :], (128, ROWS)).T[:, 0:1]
        for h in range(2):
            cols = slice(h * HALF, (h + 1) * HALF)
            t = slices[source, h].astype(F32) * column * final_gain[cols].astype(F32)[None, :]
            out[source, :, cols] = t.astype(BF16)

    finish(tp)
    for copy, other in zip(lasts, (left, right, opposite)):
        copy.wait_recv()
        landed(slices.at[other], slice_recv.at[other])
        finish(other)

    for copy in tells + flights + lasts + sum(outs, []) + sum(ons, []):
        copy.wait_send()
    sent(raw, raw_send)
    sent(routed.at[pl.ds(0, 59)], disp_send)
    sent(routed.at[pl.ds(0, 59)], ret_send)
    sent(far, far_send)
    sent(near, near_send)
    sent(slices.at[pl.ds(0, 3)], slice_send)


def local(
    tokens, norm_gain, expert_ids, group_weight, expert_logit, w_gate, w_up, w_down, final_gain
):
    anywhere = pl.BlockSpec(memory_space=pl.ANY)
    dma, groups = pltpu.SemaphoreType.DMA, PLANES * GROUP
    out = pl.pallas_call(
        kernel,
        out_shape=pltpu.VMEM((TP, ROWS, COL), BF16),
        in_specs=[anywhere] * 9,
        out_specs=pl.BlockSpec(memory_space=pltpu.VMEM),
        scratch_shapes=[
            pltpu.VMEM((ROWS, D), BF16),
            pltpu.VMEM((D,), BF16),
            pltpu.VMEM((2, ROWS), jnp.int32),
            pltpu.VMEM((1, ROWS), F32),
            pltpu.VMEM((2, ROWS), F32),
            pltpu.VMEM((COL,), BF16),
            pltpu.VMEM((TP, ROWS, COL), BF16),
            pltpu.VMEM((4, TP, ROWS, COL), BF16),
            pltpu.VMEM((5, 8, ROWS), F32),
            pltpu.VMEM((groups * CAP, ROWS), BF16),
            pltpu.VMEM((groups, CAP, D), BF16),
            pltpu.VMEM((groups, CAP, D), BF16),
            pltpu.VMEM((TP, groups * CAP, FF // TP), BF16),
            pltpu.VMEM((STAGES, groups, CAP, HALF), BF16),
            pltpu.VMEM((STAGES, groups, CAP, HALF), BF16),
            pltpu.VMEM((TP, D, FF // TP), BF16),
            pltpu.VMEM((TP, D, FF // TP), BF16),
            pltpu.VMEM((TP, TP, FF // TP, COL), BF16),
            pltpu.VMEM((ROWS, 1152), BF16),
            pltpu.VMEM((ROWS, 1152), BF16),
            pltpu.VMEM((2, STAGES, ROWS, HALF), BF16),
            pltpu.VMEM((2, STAGES, ROWS, HALF), BF16),
            pltpu.VMEM((2, STAGES, ROWS, HALF), BF16),
            pltpu.VMEM((2, STAGES, ROWS, HALF), BF16),
            pltpu.VMEM((STAGES, ROWS, HALF), BF16),
            pltpu.VMEM((TP, 2, ROWS, HALF), BF16),
            pltpu.VMEM((ROWS, 128), F32),
            pltpu.VMEM((8, ROWS), F32),
            pltpu.VMEM((TP, 8, ROWS), F32),
            dma((6,)), dma((6,)), dma((6,)), dma((6,)), dma((STAGES, 6)), dma((STAGES, 6)), dma((4,)), dma((4,)), dma, dma((4, TP)),
            dma, dma((PLANES,)), dma, dma((5, STAGES)), dma, dma((2, STAGES)), dma, dma((2, STAGES)), dma, dma((TP,)),
            dma((3,)), dma((3,)),
        ],
        compiler_params=pltpu.CompilerParams(
            collective_id=0, has_side_effects=True, vmem_limit_bytes=62 * 1024 * 1024
        ),
    )(
        tokens, norm_gain, expert_ids.T, group_weight[None, :], expert_logit.T,
        w_gate[0], w_up[0], w_down[0], final_gain,
    )
    return out.reshape(TP * ROWS, COL)


def solution(mesh):
    placed = (
        P(("ep", "tp"), None),
        P(),
        P(("ep", "tp"), None),
        P(("ep", "tp")),
        P(("ep", "tp"), None),
        P("ep", None, "tp"),
        P("ep", None, "tp"),
        P("ep", "tp", None),
        P("tp"),
    )
    return jax.shard_map(
        local, mesh=mesh, in_specs=placed, out_specs=P("ep", "tp"), check_vma=False
    )
```

```python
import jax
import jax.numpy as jnp
from jax import lax
from jax.experimental import pallas as pl
from jax.experimental.pallas import tpu as pltpu
from jax.sharding import PartitionSpec as P

D = 2048
FF = 1024
CAP = 16
ROWS = 256
PLANES = 8
GROUP = 8
LANES = GROUP * CAP
TP = 4
COL = D // TP
HALF = COL // 2
STAGES = 2 * TP
EPS = 1e-06
MESH = pl.DeviceIdType.MESH
F32 = jnp.float32
BF16 = jnp.bfloat16

A, B, C, DD, E = 0, 20, 40, 48, 56
BLOCK_A, BLOCK_B, BLOCK_C, BLOCK_D, BLOCK_E = range(5)
AT_E, AT_C, AT_D, AT_A, AT_B, AT_UP, AT_DOWN, AT_FAR = range(8)
LANE = (0, 384, 768, 896, 1024)


def kernel(
    tokens_in, gain_in, ids_in, group_weight_in, logit_in, w_gate, w_up, w_down, final_gain_in, out,
    tokens, gain, ids, group_weight, logit, final_gain,
    normed, raw, info, pick, packed, routed, hidden, product, returned, wgu, wd, high, low,
    far, far_in, near, near_in, residual, slices, squares, inverse_out, inverses,
    in_sem, own_sem, w_send, w_recv, d_send, d_recv, info_send, info_recv, raw_send, raw_recv, disp_send, disp_recv,
    ret_send, ret_recv, far_send, far_recv, near_send, near_recv, slice_send, slice_recv, inv_send, inv_recv,
):
    ep, tp = lax.axis_index("ep"), lax.axis_index("tp")
    z, inner = ep // GROUP, ep % GROUP
    up1, down1, up2, down2 = ((z + k) % PLANES for k in (1, 7, 2, 6))
    right, left, opposite = (tp + 1) % TP, (tp + 3) % TP, (tp + 2) % TP

    def remote(src, dst, send, recv, to_z, to_inner, to_tp):
        return pltpu.make_async_remote_copy(
            src_ref=src, dst_ref=dst, send_sem=send, recv_sem=recv,
            device_id={"ep": to_z * GROUP + to_inner, "tp": to_tp}, device_id_type=MESH,
        )

    def landed(dst, recv):
        remote(dst, dst, info_send, recv, z, inner, right).wait_recv()

    def sent(src, send):
        remote(src, src, send, info_recv, z, inner, right).wait_send()

    barrier = pltpu.get_barrier_semaphore()

    def greet(to_z, to_inner, to_tp):
        pl.semaphore_signal(
            barrier, inc=1, device_id={"ep": to_z * GROUP + to_inner, "tp": to_tp}, device_id_type=MESH
        )

    def greet_plane(i, _):
        o = i // GROUP
        greet((z + PLANES + (1 - 2 * (o % 2)) * (2 - o // 2)) % PLANES, i % GROUP, tp)
        return 0

    def greet_own(j, _):
        greet(z, (inner + j) % GROUP, tp)
        return 0

    lax.fori_loop(0, 4 * GROUP, greet_plane, 0)
    lax.fori_loop(1, GROUP, greet_own, 0)
    for other in (right, left, opposite):
        greet(z, inner, other)

    inputs = [
        pltpu.make_async_copy(tokens_in.at[pl.ds(n * 64, 64)], tokens.at[pl.ds(n * 64, 64)], in_sem.at[n])
        for n in range(4)
    ] + [
        pltpu.make_async_copy(src, dst, in_sem.at[4 + k])
        for k, (src, dst) in enumerate((
            (gain_in, gain), (ids_in, ids), (group_weight_in, group_weight), (logit_in, logit),
            (final_gain_in, final_gain),
        ))
    ]
    gate_part, up_part = pl.ds(0, FF // TP), pl.ds(FF // TP, FF // TP)
    own = [
        pltpu.make_async_copy(w_gate, wgu.at[tp, :, gate_part], own_sem.at[0]),
        pltpu.make_async_copy(w_up, wgu.at[tp, :, up_part], own_sem.at[1]),
    ] + [
        pltpu.make_async_copy(w_down.at[:, pl.ds(n * COL, COL)], wd.at[tp, n], own_sem.at[2 + n]) for n in range(TP)
    ]
    for copy in inputs + own[:2]:
        copy.start()
    for copy in inputs[4:]:
        copy.wait()

    def norm_rows(i, _):
        at = pl.ds(pl.multiple_of(i * 32, 32), 32)
        t = tokens[at, :].astype(F32)
        inverse = lax.rsqrt(jnp.mean(t * t, axis=-1, keepdims=True) + EPS)
        t = (t * inverse * gain[...].astype(F32)[None, :]).astype(BF16)
        for n in range(TP):
            normed[n, at, :] = t[:, n * COL:(n + 1) * COL]
        return 0

    for n in range(4):
        inputs[n].wait()
        lax.fori_loop(2 * n, 2 * n + 2, norm_rows, 0)

    for copy in own[:2]:
        copy.wait()
    pl.semaphore_wait(barrier, 42)

    def weights(q, part, k, to):
        block = wgu.at[q, :, part]
        copy = remote(block, block, w_send, w_recv.at[k], z, inner, to)
        copy.start()
        return copy

    flights = [
        weights(tp, gate_part, 0, right),
        weights(tp, up_part, 1, left),
        weights(tp, up_part, 2, right),
        weights(tp, gate_part, 3, left),
    ]
    for copy in own[2:]:
        copy.start()

    id0, id1 = ids[0:1, :], ids[1:2, :]
    lane = lax.broadcasted_iota(jnp.int32, (PLANES * GROUP, ROWS), 0)
    first, second = lane == id0, lane == id1
    named = jnp.where(first, 1.0, jnp.where(second, 1.0, 0.0)).astype(BF16)
    earlier = jnp.where(
        lax.broadcasted_iota(jnp.int32, (ROWS, ROWS), 0)
        < lax.broadcasted_iota(jnp.int32, (ROWS, ROWS), 1), 1.0, 0.0,
    ).astype(BF16)
    before = jnp.dot(named, earlier, preferred_element_type=F32)
    e0, e1 = jnp.exp(logit[0:1, :]), jnp.exp(logit[1:2, :])
    total = e0 + e1
    info[BLOCK_E, 0:1, :] = id0.astype(F32) * CAP + jnp.sum(jnp.where(first, before, 0.0), axis=0, keepdims=True)
    info[BLOCK_E, 1:2, :] = id1.astype(F32) * CAP + jnp.sum(jnp.where(second, before, 0.0), axis=0, keepdims=True)
    info[BLOCK_E, 2:3, :] = group_weight[...] * (e0 / total)
    info[BLOCK_E, 3:4, :] = group_weight[...] * (e1 / total)
    info[BLOCK_E, 4:8, :] = jnp.zeros((4, ROWS), F32)

    sections = {
        BLOCK_A: ((0, 128, z * LANES, 1), (128, 128, up1 * LANES, 1), (256, 64, up2 * LANES, 2)),
        BLOCK_B: ((0, 128, z * LANES, 1), (128, 128, down1 * LANES, 1), (256, 64, down2 * LANES + CAP, 2)),
        BLOCK_C: ((0, 128, z * LANES, 1),),
        BLOCK_D: ((0, 128, z * LANES, 1),),
        BLOCK_E: ((0, 128, z * LANES, 1),),
    }

    def slots(count, number, step):
        row = lax.broadcasted_iota(jnp.int32, (count, ROWS), 0)
        return (row + (step - 1) * CAP * lax.div(row, CAP) + number).astype(F32)

    first_group = {BLOCK_A: A, BLOCK_B: B, BLOCK_C: C, BLOCK_D: DD, BLOCK_E: E}

    def make_pick(block):
        at0, at1 = info[block, 0:1, :], info[block, 1:2, :]
        for start, count, number, step in sections[block]:
            slot = slots(count, number, step)
            row = first_group[block] * CAP + start
            pick[row:row + count, :] = jnp.where(slot == at0, 1.0, jnp.where(slot == at1, 1.0, 0.0)).astype(BF16)

    def make_weights(block):
        at0, at1, w0, w1 = (info[block, k:k + 1, :] for k in range(4))
        for start, count, number, step in sections[block]:
            slot = slots(128, number, step)
            w = (jnp.where(slot == at0, w0, 0.0) + jnp.where(slot == at1, w1, 0.0)).T[:, :count]
            top_term = w.astype(BF16)
            lanes = slice(LANE[block] + start, LANE[block] + start + count)
            high[:, lanes] = top_term
            low[:, lanes] = (w - top_term.astype(F32)).astype(BF16)

    def pack(block, groups, src, n):
        row = first_group[block] * CAP
        rows = jnp.dot(pick[row:row + groups * CAP, :], src, preferred_element_type=F32).astype(BF16)
        packed[pl.ds(first_group[block], groups), :, pl.ds(pl.multiple_of(n * COL, COL), COL)] = rows.reshape(
            groups, CAP, COL
        )

    def send_own_plane(ways, n):
        cols = pl.ds(pl.multiple_of(n * COL, COL), COL)

        def send(j, _):
            to = (inner + j) % GROUP
            for block, at in ways:
                remote(
                    packed.at[first_group[block] + to, :, cols], routed.at[at * GROUP + inner, :, cols], disp_send,
                    disp_recv.at[at], z, to, tp,
                ).start()
            return 0

        lax.fori_loop(1, GROUP, send, 0)
        for block, at in ways:
            routed[at * GROUP + inner, :, cols] = packed[first_group[block] + inner, :, cols]

    tells = [
        remote(info.at[BLOCK_E], info.at[block], info_send, info_recv, to, inner, tp)
        for block, to in ((BLOCK_C, up1), (BLOCK_D, down1), (BLOCK_A, up2), (BLOCK_B, down2))
    ]
    for copy in tells:
        copy.start()

    def hop_out(n, _):
        remote(normed.at[n], raw.at[0, n], raw_send, raw_recv.at[0, n], up1, inner, tp).start()
        remote(normed.at[n], raw.at[1, n], raw_send, raw_recv.at[0, n], down1, inner, tp).start()
        return 0

    lax.fori_loop(0, TP, hop_out, 0)

    make_pick(BLOCK_E)

    def pack_own(n, _):
        pack(BLOCK_E, 8, normed[n], n)
        send_own_plane(((BLOCK_E, AT_E),), n)
        return 0

    lax.fori_loop(0, TP, pack_own, 0)
    landed(info.at[pl.ds(0, 4)], info_recv)
    for block in (BLOCK_C, BLOCK_D, BLOCK_A, BLOCK_B):
        make_pick(block)

    def hop_on(n, _):
        landed(raw.at[0, pl.ds(0, 2)], raw_recv.at[0, n])
        remote(raw.at[0, n], raw.at[2, n], raw_send, raw_recv.at[1, n], up1, inner, tp).start()
        remote(raw.at[1, n], raw.at[3, n], raw_send, raw_recv.at[1, n], down1, inner, tp).start()
        pack(BLOCK_C, 8, raw[0, n], n)
        pack(BLOCK_D, 8, raw[1, n], n)
        send_own_plane(((BLOCK_C, AT_C), (BLOCK_D, AT_D)), n)
        return 0

    lax.fori_loop(0, TP, hop_on, 0)

    half = FF // TP // 2
    top, bottom = pl.ds(0, half), pl.ds(half, half)

    def over_y(q, piece, part, k, to):
        block = wd.at[q, piece % TP, part, pl.ds(piece // TP * HALF, HALF)]
        return remote(block, block, d_send, d_recv.at[piece, k], z, inner, to)

    def down_out(piece):
        return [
            over_y(tp, piece, top, 0, right), over_y(tp, piece, bottom, 0, left),
            over_y(tp, piece, bottom, 1, right), over_y(tp, piece, top, 1, left),
        ]

    def down_on(piece):
        return [over_y(left, piece, top, 1, right), over_y(right, piece, bottom, 1, left)]

    def start(copies):
        for copy in copies:
            copy.start()

    flights[0].wait_recv()
    flights.append(weights(left, gate_part, 4, right))
    flights[1].wait_recv()
    flights.append(weights(right, up_part, 5, left))
    outs, ons = [down_out(k) for k in range(STAGES)], [down_on(k) for k in range(STAGES)]
    for copy in own[2:]:
        copy.wait()
    start(outs[0])

    def relay_down(k):
        landed(wd.at[0, 0, :, pl.ds(0, HALF)], d_recv.at[k, 0])
        start(ons[k])
        for later in ((1,), (2,), (3, 4), (5,), (6,), (7,), (), ())[k]:
            start(outs[later])

    def expand(q, first_row, count):
        groups = count // CAP
        xs = routed[pl.ds(first_row // CAP, groups)].reshape(count, D)
        both = jnp.dot(xs, wgu[q], preferred_element_type=F32)
        g, u = both[:, :FF // TP], both[:, FF // TP:]
        hidden[q, pl.ds(first_row, count), :] = (g / (1.0 + jnp.exp(-g)) * u).astype(BF16)

    def expand_of(order, first_row, count):
        def part(i, _):
            expand((tp + order[0] + order[1] * i) % TP, first_row, count)
            return 0

        lax.fori_loop(0, order[2], part, 0)

    def rows_landed(at, groups):
        landed(routed.at[pl.ds(0, groups)], disp_recv.at[at])

    for block in range(5):
        make_weights(block)
    rows_landed(AT_E, GROUP - 1)
    rows_landed(AT_C, GROUP - 1)
    rows_landed(AT_D, GROUP - 1)
    expand_of((0, 0, 1), 0, 384)

    def hop_last(n, _):
        landed(raw.at[0, pl.ds(0, 2)], raw_recv.at[1, n])
        pack(BLOCK_A, 20, raw[2, n], n)
        pack(BLOCK_B, 20, raw[3, n], n)
        send_own_plane(((BLOCK_A, AT_A), (BLOCK_B, AT_B)), n)
        cols = pl.ds(pl.multiple_of(n * COL, COL), COL)

        def send_next(i, _):
            remote(
                packed.at[A + 8 + i, :, cols], routed.at[AT_UP * GROUP + inner, :, cols], disp_send,
                disp_recv.at[AT_UP], up1, i, tp,
            ).start()
            remote(
                packed.at[B + 8 + i, :, cols], routed.at[AT_DOWN * GROUP + inner, :, cols], disp_send,
                disp_recv.at[AT_DOWN], down1, i, tp,
            ).start()
            return 0

        def send_far(i, _):
            remote(
                packed.at[A + 16 + i, :, cols], routed.at[AT_FAR * GROUP + inner, :, cols], disp_send,
                disp_recv.at[AT_FAR], up2, 2 * i, tp,
            ).start()
            remote(
                packed.at[B + 16 + i, :, cols], routed.at[AT_FAR * GROUP + inner, :, cols], disp_send,
                disp_recv.at[AT_FAR], down2, 2 * i + 1, tp,
            ).start()
            return 0

        lax.fori_loop(0, 4, send_far, 0)
        lax.fori_loop(0, GROUP, send_next, 0)
        return 0

    lax.fori_loop(0, TP, hop_last, 0)

    flights[2].wait_recv()
    flights[3].wait_recv()
    expand_of((1, 2, 2), 0, 384)
    rows_landed(AT_A, GROUP - 1)
    rows_landed(AT_B, GROUP - 1)
    expand_of((3, 1, 3), 384, 256)
    flights[4].wait_recv()
    flights[5].wait_recv()
    expand_of((2, 0, 1), 0, 640)
    relay_down(0)
    rows_landed(AT_UP, GROUP)
    rows_landed(AT_DOWN, GROUP)
    rows_landed(AT_FAR, GROUP)
    expand_of((0, 1, 4), 640, 384)

    def columns_at(k):
        if k < TP:
            return k, 0
        if k < STAGES - 1:
            return k - TP + (k - tp) // TP, 1
        return tp, 1

    odd = inner % 2
    ways = ((AT_A, BLOCK_A), (AT_B, BLOCK_B), (AT_C, BLOCK_C), (AT_D, BLOCK_D), (AT_E, BLOCK_E))

    def contract(k):
        n, h = columns_at(k)
        cols = pl.ds(h * HALF, HALF)
        for piece in ((0,), (1,), (2,), (3,), (4, 5), (6,), (7,), ())[k]:
            landed(wd.at[0, 0], d_recv.at[piece, 1])

        def part(i, _):
            i = 3 - i
            at = pl.ds(pl.multiple_of(i * 256, 256), 256)
            rows = jnp.dot(hidden[0, at, :], wd[0, n, :, cols], preferred_element_type=F32)
            for q in range(1, TP):
                rows += jnp.dot(hidden[q, at, :], wd[q, n, :, cols], preferred_element_type=F32)
            product[k, pl.ds(i * 16, 16)] = rows.astype(BF16).reshape(16, CAP, HALF)
            return 0

        lax.fori_loop(0, 2, part, 0)

        def send_far(i, _):
            answer(k, AT_FAR, A + 16 + inner // 2 + (B - A) * odd, BLOCK_A, (z + 6 + 4 * odd) % PLANES, i)
            answer(k, AT_UP, A + 8 + inner, BLOCK_A, down1, i)
            answer(k, AT_DOWN, B + 8 + inner, BLOCK_B, up1, i)
            return 0

        lax.fori_loop(0, GROUP, send_far, 0)
        lax.fori_loop(2, 4, part, 0)
        answer_plane(k, ways[0:2])

    def answer(k, at, group, block, to_z, i):
        remote(product.at[k, at * GROUP + i], returned.at[k, group], ret_send, ret_recv.at[block // 2, k], to_z, i, tp).start()

    def answer_plane(k, some):
        def send_own(j, _):
            to = (inner + j) % GROUP
            for at, block in some:
                answer(k, at, first_group[block] + inner, block, z, to)
            return 0

        lax.fori_loop(1, GROUP, send_own, 0)
        for at, block in some:
            returned[k, first_group[block] + inner] = product[k, at * GROUP + inner]

    def answer_near(k):
        answer_plane(k, ways[2:4])
        answer_plane(k, ways[4:5])

    def weighed(block, groups, k):
        rows = returned[k, pl.ds(first_group[block], groups)].reshape(groups * CAP, HALF)
        lanes = slice(LANE[block], LANE[block] + groups * CAP)
        return jnp.dot(high[:, lanes], rows, preferred_element_type=F32) + jnp.dot(
            low[:, lanes], rows, preferred_element_type=F32
        )

    def send_partials(k):
        landed(returned.at[k, pl.ds(0, 38)], ret_recv.at[0, k])
        far[0, k] = weighed(BLOCK_A, 20, k).astype(BF16)
        remote(far.at[0, k], far_in.at[0, k], far_send, far_recv.at[k], down1, inner, tp).start()
        far[1, k] = weighed(BLOCK_B, 20, k).astype(BF16)
        remote(far.at[1, k], far_in.at[1, k], far_send, far_recv.at[k], up1, inner, tp).start()

    def add_partials(k):
        landed(returned.at[k, pl.ds(0, 14)], ret_recv.at[1, k])
        landed(far_in.at[0, pl.ds(0, 2)], far_recv.at[k])
        for side, block, to in ((0, BLOCK_C, down1), (1, BLOCK_D, up1)):
            here = weighed(block, 8, k)
            near[side, k] = (here + far_in[side, k].astype(F32)).astype(BF16)
            remote(near.at[side, k], near_in.at[side, k], near_send, near_recv.at[k], to, inner, tp).start()

    def close(k):
        n, h = columns_at(k)
        landed(returned.at[k, pl.ds(0, 7)], ret_recv.at[2, k])
        here = weighed(BLOCK_E, 8, k)
        landed(near_in.at[0, pl.ds(0, 2)], near_recv.at[k])
        t = tokens[:, pl.ds(pl.multiple_of(n * COL + h * HALF, HALF), HALF)].astype(F32)
        r = (t + here + near_in[0, k].astype(F32) + near_in[1, k].astype(F32)).astype(BF16)
        residual[k] = r
        s = r.astype(F32)
        s = s * s
        s = s[:, 0:128] + s[:, 128:256]
        squares[...] = s if k == 0 else squares[...] + s

        @pl.when(n != tp)
        def _():
            remote(residual.at[k], slices.at[tp, h], slice_send, slice_recv.at[tp], z, inner, n).start()

        @pl.when(n == tp)
        def _():
            slices[tp, h] = residual[k]

    relay_down(1)
    contract(0)
    contract(1)
    answer_near(0)
    relay_down(2)
    answer_near(1)
    send_partials(0)
    contract(2)
    relay_down(3)
    send_partials(1)
    answer_near(2)
    contract(3)
    relay_down(4)
    answer_near(3)
    add_partials(0)
    send_partials(2)
    relay_down(5)
    add_partials(1)
    relay_down(6)
    close(0)
    contract(4)
    relay_down(7)
    answer_near(4)
    send_partials(3)
    add_partials(2)
    close(1)
    contract(5)
    answer_near(5)
    send_partials(4)
    add_partials(3)
    close(2)
    contract(6)
    answer_near(6)
    send_partials(5)
    add_partials(4)
    close(3)
    contract(7)
    answer_near(7)
    send_partials(6)
    add_partials(5)
    close(4)
    send_partials(7)
    add_partials(6)
    close(5)
    add_partials(7)
    close(6)
    close(7)

    inverse = lax.rsqrt(jnp.sum(squares[...], axis=-1, keepdims=True) / D + EPS)
    inverse_out[...] = jnp.broadcast_to(inverse, (ROWS, 128)).T[0:8, :]
    lasts = [
        remote(inverse_out, inverses.at[tp], inv_send, inv_recv.at[k], z, inner, other)
        for k, other in enumerate((right, left, opposite))
    ]
    start(lasts)
    inverses[tp] = inverse_out[...]

    def finish(source):
        column = jnp.broadcast_to(inverses[source, 0:1, :], (128, ROWS)).T[:, 0:1]
        for h in range(2):
            cols = slice(h * HALF, (h + 1) * HALF)
            t = slices[source, h].astype(F32) * column * final_gain[cols].astype(F32)[None, :]
            out[source, :, cols] = t.astype(BF16)

    finish(tp)
    for copy, other in zip(lasts, (left, right, opposite)):
        copy.wait_recv()
        landed(slices.at[other], slice_recv.at[other])
        finish(other)

    sent(info.at[pl.ds(0, 4)], info_send)
    sent(wgu.at[pl.ds(0, 3)], w_send)
    sent(wd.at[pl.ds(0, 3)], d_send)
    sent(inverses.at[pl.ds(0, 3)], inv_send)
    sent(raw, raw_send)
    sent(routed.at[pl.ds(0, 59)], disp_send)
    sent(routed.at[pl.ds(0, 59)], ret_send)
    sent(far, far_send)
    sent(near, near_send)
    sent(slices.at[pl.ds(0, 3)], slice_send)


def local(
    tokens, norm_gain, expert_ids, group_weight, expert_logit, w_gate, w_up, w_down, final_gain
):
    anywhere = pl.BlockSpec(memory_space=pl.ANY)
    dma, groups = pltpu.SemaphoreType.DMA, PLANES * GROUP
    out = pl.pallas_call(
        kernel,
        out_shape=pltpu.VMEM((TP, ROWS, COL), BF16),
        in_specs=[anywhere] * 9,
        out_specs=pl.BlockSpec(memory_space=pltpu.VMEM),
        scratch_shapes=[
            pltpu.VMEM((ROWS, D), BF16),
            pltpu.VMEM((D,), BF16),
            pltpu.VMEM((2, ROWS), jnp.int32),
            pltpu.VMEM((1, ROWS), F32),
            pltpu.VMEM((2, ROWS), F32),
            pltpu.VMEM((COL,), BF16),
            pltpu.VMEM((TP, ROWS, COL), BF16),
            pltpu.VMEM((4, TP, ROWS, COL), BF16),
            pltpu.VMEM((5, 8, ROWS), F32),
            pltpu.VMEM((groups * CAP, ROWS), BF16),
            pltpu.VMEM((groups, CAP, D), BF16),
            pltpu.VMEM((groups, CAP, D), BF16),
            pltpu.VMEM((TP, groups * CAP, FF // TP), BF16),
            pltpu.VMEM((STAGES, groups, CAP, HALF), BF16),
            pltpu.VMEM((STAGES, groups, CAP, HALF), BF16),
            pltpu.VMEM((TP, D, 2 * FF // TP), BF16),
            pltpu.VMEM((TP, TP, FF // TP, COL), BF16),
            pltpu.VMEM((ROWS, 1152), BF16),
            pltpu.VMEM((ROWS, 1152), BF16),
            pltpu.VMEM((2, STAGES, ROWS, HALF), BF16),
            pltpu.VMEM((2, STAGES, ROWS, HALF), BF16),
            pltpu.VMEM((2, STAGES, ROWS, HALF), BF16),
            pltpu.VMEM((2, STAGES, ROWS, HALF), BF16),
            pltpu.VMEM((STAGES, ROWS, HALF), BF16),
            pltpu.VMEM((TP, 2, ROWS, HALF), BF16),
            pltpu.VMEM((ROWS, 128), F32),
            pltpu.VMEM((8, ROWS), F32),
            pltpu.VMEM((TP, 8, ROWS), F32),
            dma((9,)), dma((6,)), dma, dma((6,)), dma, dma((STAGES, 2)), dma, dma, dma, dma((2, TP)),
            dma, dma((PLANES,)), dma, dma((3, STAGES)), dma, dma((STAGES,)), dma, dma((STAGES,)), dma, dma((TP,)),
            dma, dma((3,)),
        ],
        compiler_params=pltpu.CompilerParams(
            collective_id=0, has_side_effects=True, vmem_limit_bytes=62 * 1024 * 1024
        ),
    )(
        tokens, norm_gain, expert_ids.T, group_weight[None, :], expert_logit.T,
        w_gate[0], w_up[0], w_down[0], final_gain,
    )
    return out.reshape(TP * ROWS, COL)


def solution(mesh):
    placed = (
        P(("ep", "tp"), None),
        P(),
        P(("ep", "tp"), None),
        P(("ep", "tp")),
        P(("ep", "tp"), None),
        P("ep", None, "tp"),
        P("ep", None, "tp"),
        P("ep", "tp", None),
        P("tp"),
    )
    return jax.shard_map(
        local, mesh=mesh, in_specs=placed, out_specs=P("ep", "tp"), check_vma=False
    )
```

```python
import jax
import jax.numpy as jnp
from jax import lax
from jax.experimental import pallas as pl
from jax.experimental.pallas import tpu as pltpu
from jax.sharding import PartitionSpec as P

D = 2048
FF = 1024
CAP = 16
ROWS = 256
PLANES = 8
GROUP = 8
LANES = GROUP * CAP
TP = 4
COL = D // TP
HALF = COL // 2
STAGES = 2 * TP
EPS = 1e-06
MESH = pl.DeviceIdType.MESH
F32 = jnp.float32
BF16 = jnp.bfloat16

A, B, C, DD, E = 0, 20, 40, 48, 56
BLOCK_A, BLOCK_B, BLOCK_C, BLOCK_D, BLOCK_E = range(5)
AT_E, AT_C, AT_D, AT_A, AT_B, AT_UP, AT_DOWN, AT_FAR = range(8)
LANE = (0, 384, 768, 896, 1024)


def kernel(
    tokens_in, gain_in, ids_in, group_weight_in, logit_in, w_gate, w_up, w_down, final_gain_in, out,
    tokens, gain, ids, group_weight, logit, final_gain,
    normed, raw, info, pick, packed, routed, hidden, product, returned, wgu, wd, high, low,
    far, far_in, near, near_in, residual, slices, squares, inverse_out, inverses,
    in_sem, own_sem, w_send, w_recv, d_send, d_recv, info_send, info_recv, raw_send, raw_recv, disp_send, disp_recv,
    ret_send, ret_recv, far_send, far_recv, near_send, near_recv, slice_send, slice_recv, inv_send, inv_recv,
):
    ep, tp = lax.axis_index("ep"), lax.axis_index("tp")
    z, inner = ep // GROUP, ep % GROUP
    up1, down1, up2, down2 = ((z + k) % PLANES for k in (1, 7, 2, 6))
    right, left, opposite = (tp + 1) % TP, (tp + 3) % TP, (tp + 2) % TP

    def remote(src, dst, send, recv, to_z, to_inner, to_tp):
        return pltpu.make_async_remote_copy(
            src_ref=src, dst_ref=dst, send_sem=send, recv_sem=recv,
            device_id={"ep": to_z * GROUP + to_inner, "tp": to_tp}, device_id_type=MESH,
        )

    def landed(dst, recv):
        remote(dst, dst, info_send, recv, z, inner, right).wait_recv()

    def sent(src, send):
        remote(src, src, send, info_recv.at[0], z, inner, right).wait_send()

    def start(copies):
        for copy in copies:
            copy.start()

    barrier = pltpu.get_barrier_semaphore()

    def greet(to_z, to_inner, to_tp):
        pl.semaphore_signal(
            barrier, inc=1, device_id={"ep": to_z * GROUP + to_inner, "tp": to_tp}, device_id_type=MESH
        )

    def greet_own(j, _):
        greet(z, (inner + j) % GROUP, tp)
        return 0

    greet(up1, inner, tp)
    greet(down1, inner, tp)
    lax.fori_loop(1, GROUP, greet_own, 0)
    for other in (opposite, right, left):
        greet(z, inner, other)

    inputs = [
        pltpu.make_async_copy(tokens_in.at[pl.ds(n * 64, 64)], tokens.at[pl.ds(n * 64, 64)], in_sem.at[n])
        for n in range(4)
    ] + [
        pltpu.make_async_copy(src, dst, in_sem.at[4 + k])
        for k, (src, dst) in enumerate((
            (gain_in, gain), (ids_in, ids), (group_weight_in, group_weight), (logit_in, logit),
            (final_gain_in, final_gain),
        ))
    ]
    gate_part, up_part = pl.ds(0, FF // TP), pl.ds(FF // TP, FF // TP)
    own = [
        pltpu.make_async_copy(w_gate, wgu.at[tp, :, gate_part], own_sem.at[0]),
        pltpu.make_async_copy(w_up, wgu.at[tp, :, up_part], own_sem.at[1]),
    ] + [
        pltpu.make_async_copy(w_down.at[:, pl.ds(n * COL, COL)], wd.at[tp, n], own_sem.at[2 + n]) for n in range(TP)
    ]
    for copy in inputs + own[:2]:
        copy.start()
    for copy in inputs[4:]:
        copy.wait()

    def norm_rows(i, _):
        at = pl.ds(pl.multiple_of(i * 32, 32), 32)
        t = tokens[at, :].astype(F32)
        inverse = lax.rsqrt(jnp.mean(t * t, axis=-1, keepdims=True) + EPS)
        t = (t * inverse * gain[...].astype(F32)[None, :]).astype(BF16)
        for n in range(TP):
            normed[n, at, :] = t[:, n * COL:(n + 1) * COL]
        return 0

    for n in range(4):
        inputs[n].wait()
        lax.fori_loop(2 * n, 2 * n + 2, norm_rows, 0)

    for copy in own[:2]:
        copy.wait()
    pl.semaphore_wait(barrier, 12)

    def weights(q, part, k, to):
        block = wgu.at[q, :, part]
        copy = remote(block, block, w_send, w_recv.at[k], z, inner, to)
        copy.start()
        return copy

    flights = [
        weights(tp, gate_part, 0, right),
        weights(tp, up_part, 1, left),
        weights(tp, up_part, 2, right),
        weights(tp, gate_part, 3, left),
    ]
    for copy in own[2:]:
        copy.start()

    id0, id1 = ids[0:1, :], ids[1:2, :]
    lane = lax.broadcasted_iota(jnp.int32, (PLANES * GROUP, ROWS), 0)
    first, second = lane == id0, lane == id1
    named = jnp.where(first, 1.0, jnp.where(second, 1.0, 0.0)).astype(BF16)
    earlier = jnp.where(
        lax.broadcasted_iota(jnp.int32, (ROWS, ROWS), 0)
        < lax.broadcasted_iota(jnp.int32, (ROWS, ROWS), 1), 1.0, 0.0,
    ).astype(BF16)
    before = jnp.dot(named, earlier, preferred_element_type=F32)
    e0, e1 = jnp.exp(logit[0:1, :]), jnp.exp(logit[1:2, :])
    total = e0 + e1
    info[BLOCK_E, 0:1, :] = id0.astype(F32) * CAP + jnp.sum(jnp.where(first, before, 0.0), axis=0, keepdims=True)
    info[BLOCK_E, 1:2, :] = id1.astype(F32) * CAP + jnp.sum(jnp.where(second, before, 0.0), axis=0, keepdims=True)
    info[BLOCK_E, 2:3, :] = group_weight[...] * (e0 / total)
    info[BLOCK_E, 3:4, :] = group_weight[...] * (e1 / total)
    info[BLOCK_E, 4:8, :] = jnp.zeros((4, ROWS), F32)

    sections = {
        BLOCK_A: ((0, 128, z * LANES, 1), (128, 128, up1 * LANES, 1), (256, 64, up2 * LANES, 2)),
        BLOCK_B: ((0, 128, z * LANES, 1), (128, 128, down1 * LANES, 1), (256, 64, down2 * LANES + CAP, 2)),
        BLOCK_C: ((0, 128, z * LANES, 1),),
        BLOCK_D: ((0, 128, z * LANES, 1),),
        BLOCK_E: ((0, 128, z * LANES, 1),),
    }

    def slots(count, number, step):
        row = lax.broadcasted_iota(jnp.int32, (count, ROWS), 0)
        return (row + (step - 1) * CAP * lax.div(row, CAP) + number).astype(F32)

    first_group = {BLOCK_A: A, BLOCK_B: B, BLOCK_C: C, BLOCK_D: DD, BLOCK_E: E}

    def make_pick(block):
        at0, at1 = info[block, 0:1, :], info[block, 1:2, :]
        for start, count, number, step in sections[block]:
            slot = slots(count, number, step)
            row = first_group[block] * CAP + start
            pick[row:row + count, :] = jnp.where(slot == at0, 1.0, jnp.where(slot == at1, 1.0, 0.0)).astype(BF16)

    def make_weights(block):
        at0, at1, w0, w1 = (info[block, k:k + 1, :] for k in range(4))
        for start, count, number, step in sections[block]:
            slot = slots(128, number, step)
            w = (jnp.where(slot == at0, w0, 0.0) + jnp.where(slot == at1, w1, 0.0)).T[:, :count]
            top_term = w.astype(BF16)
            lanes = slice(LANE[block] + start, LANE[block] + start + count)
            high[:, lanes] = top_term
            low[:, lanes] = (w - top_term.astype(F32)).astype(BF16)

    def pack(block, groups, src, n):
        row = first_group[block] * CAP
        rows = jnp.dot(pick[row:row + groups * CAP, :], src, preferred_element_type=F32).astype(BF16)
        packed[pl.ds(first_group[block], groups), :, pl.ds(pl.multiple_of(n * COL, COL), COL)] = rows.reshape(
            groups, CAP, COL
        )

    def send_own_plane(ways, n):
        cols = pl.ds(pl.multiple_of(n * COL, COL), COL)

        def send(j, _):
            to = (inner + j) % GROUP
            for block, at in ways:
                remote(
                    packed.at[first_group[block] + to, :, cols], routed.at[at * GROUP + inner, :, cols], disp_send,
                    disp_recv.at[at], z, to, tp,
                ).start()
            return 0

        lax.fori_loop(1, GROUP, send, 0)
        for block, at in ways:
            routed[at * GROUP + inner, :, cols] = packed[first_group[block] + inner, :, cols]

    def tell(block, to, at, k):
        return remote(info.at[block], info.at[at], info_send, info_recv.at[k], to, inner, tp)

    start([tell(BLOCK_E, up1, BLOCK_C, 0), tell(BLOCK_E, down1, BLOCK_D, 0)])

    def hop_out(n, _):
        remote(normed.at[n], raw.at[0, n], raw_send, raw_recv.at[0, n], up1, inner, tp).start()
        remote(normed.at[n], raw.at[1, n], raw_send, raw_recv.at[0, n], down1, inner, tp).start()
        return 0

    lax.fori_loop(0, TP, hop_out, 0)

    make_pick(BLOCK_E)

    def pack_own(n, _):
        pack(BLOCK_E, 8, normed[n], n)
        send_own_plane(((BLOCK_E, AT_E),), n)
        return 0

    lax.fori_loop(0, TP, pack_own, 0)
    landed(info.at[pl.ds(0, 2)], info_recv.at[0])
    start([tell(BLOCK_C, up1, BLOCK_A, 1), tell(BLOCK_D, down1, BLOCK_B, 1)])
    for block in (BLOCK_C, BLOCK_D):
        make_pick(block)

    def hop_on(n, _):
        landed(raw.at[0, pl.ds(0, 2)], raw_recv.at[0, n])
        remote(raw.at[0, n], raw.at[2, n], raw_send, raw_recv.at[1, n], up1, inner, tp).start()
        remote(raw.at[1, n], raw.at[3, n], raw_send, raw_recv.at[1, n], down1, inner, tp).start()
        pack(BLOCK_C, 8, raw[0, n], n)
        pack(BLOCK_D, 8, raw[1, n], n)
        send_own_plane(((BLOCK_C, AT_C), (BLOCK_D, AT_D)), n)
        return 0

    lax.fori_loop(0, TP, hop_on, 0)

    half = FF // TP // 2
    top, bottom = pl.ds(0, half), pl.ds(half, half)

    def over_y(q, piece, part, k, to):
        block = wd.at[q, piece % TP, part, pl.ds(piece // TP * HALF, HALF)]
        return remote(block, block, d_send, d_recv.at[piece, k], z, inner, to)

    def down_out(piece):
        return [
            over_y(tp, piece, top, 0, right), over_y(tp, piece, bottom, 0, left),
            over_y(tp, piece, bottom, 1, right), over_y(tp, piece, top, 1, left),
        ]

    def down_on(piece):
        return [over_y(left, piece, top, 1, right), over_y(right, piece, bottom, 1, left)]

    flights[0].wait_recv()
    flights.append(weights(left, gate_part, 4, right))
    flights[1].wait_recv()
    flights.append(weights(right, up_part, 5, left))
    outs, ons = [down_out(k) for k in range(STAGES)], [down_on(k) for k in range(STAGES)]
    for copy in own[2:]:
        copy.wait()
    start(outs[0])

    def relay_down(k):
        landed(wd.at[0, 0, :, pl.ds(0, HALF)], d_recv.at[k, 0])
        start(ons[k])
        for later in ((1,), (2,), (3, 4), (5,), (6,), (7,), (), ())[k]:
            start(outs[later])

    def expand(q, first_row, count):
        groups = count // CAP
        xs = routed[pl.ds(first_row // CAP, groups)].reshape(count, D)
        both = jnp.dot(xs, wgu[q], preferred_element_type=F32)
        g, u = both[:, :FF // TP], both[:, FF // TP:]
        hidden[q, pl.ds(first_row, count), :] = (g / (1.0 + jnp.exp(-g)) * u).astype(BF16)

    def expand_of(order, first_row, count):
        def part(i, _):
            expand((tp + order[0] + order[1] * i) % TP, first_row, count)
            return 0

        lax.fori_loop(0, order[2], part, 0)

    def rows_landed(at, groups):
        landed(routed.at[pl.ds(0, groups)], disp_recv.at[at])

    landed(info.at[pl.ds(0, 2)], info_recv.at[1])
    for block in (BLOCK_A, BLOCK_B):
        make_pick(block)
    for block in range(5):
        make_weights(block)
    rows_landed(AT_E, GROUP - 1)
    rows_landed(AT_C, GROUP - 1)
    rows_landed(AT_D, GROUP - 1)
    expand_of((0, 0, 1), 0, 384)

    def hop_last(n, _):
        landed(raw.at[0, pl.ds(0, 2)], raw_recv.at[1, n])
        pack(BLOCK_A, 20, raw[2, n], n)
        pack(BLOCK_B, 20, raw[3, n], n)
        send_own_plane(((BLOCK_A, AT_A), (BLOCK_B, AT_B)), n)
        cols = pl.ds(pl.multiple_of(n * COL, COL), COL)

        def send_next(i, _):
            remote(
                packed.at[A + 8 + i, :, cols], routed.at[AT_UP * GROUP + inner, :, cols], disp_send,
                disp_recv.at[AT_UP], up1, i, tp,
            ).start()
            remote(
                packed.at[B + 8 + i, :, cols], routed.at[AT_DOWN * GROUP + inner, :, cols], disp_send,
                disp_recv.at[AT_DOWN], down1, i, tp,
            ).start()
            return 0

        def send_far(i, _):
            remote(
                packed.at[A + 16 + i, :, cols], routed.at[AT_FAR * GROUP + inner, :, cols], disp_send,
                disp_recv.at[AT_FAR], up2, 2 * i, tp,
            ).start()
            remote(
                packed.at[B + 16 + i, :, cols], routed.at[AT_FAR * GROUP + inner, :, cols], disp_send,
                disp_recv.at[AT_FAR], down2, 2 * i + 1, tp,
            ).start()
            return 0

        lax.fori_loop(0, 4, send_far, 0)
        lax.fori_loop(0, GROUP, send_next, 0)
        return 0

    lax.fori_loop(0, TP, hop_last, 0)

    flights[2].wait_recv()
    flights[3].wait_recv()
    expand_of((1, 2, 2), 0, 384)
    rows_landed(AT_A, GROUP - 1)
    rows_landed(AT_B, GROUP - 1)
    expand_of((3, 1, 3), 384, 256)
    flights[4].wait_recv()
    flights[5].wait_recv()
    expand_of((2, 0, 1), 0, 640)
    relay_down(0)
    rows_landed(AT_UP, GROUP)
    rows_landed(AT_DOWN, GROUP)
    rows_landed(AT_FAR, GROUP)
    expand_of((0, 1, 4), 640, 384)

    def columns_at(k):
        if k < TP:
            return k, 0
        if k < STAGES - 1:
            return k - TP + (k - tp) // TP, 1
        return tp, 1

    odd = inner % 2
    ways = ((AT_A, BLOCK_A), (AT_B, BLOCK_B), (AT_C, BLOCK_C), (AT_D, BLOCK_D), (AT_E, BLOCK_E))

    def contract(k):
        n, h = columns_at(k)
        cols = pl.ds(h * HALF, HALF)
        for piece in ((0,), (1,), (2,), (3,), (4, 5), (6,), (7,), ())[k]:
            landed(wd.at[0, 0], d_recv.at[piece, 1])

        def part(i, _):
            i = 3 - i
            at = pl.ds(pl.multiple_of(i * 256, 256), 256)
            rows = jnp.dot(hidden[0, at, :], wd[0, n, :, cols], preferred_element_type=F32)
            for q in range(1, TP):
                rows += jnp.dot(hidden[q, at, :], wd[q, n, :, cols], preferred_element_type=F32)
            product[k, pl.ds(i * 16, 16)] = rows.astype(BF16).reshape(16, CAP, HALF)
            return 0

        lax.fori_loop(0, 2, part, 0)

        def send_far(i, _):
            answer(k, AT_FAR, A + 16 + inner // 2 + (B - A) * odd, BLOCK_A, (z + 6 + 4 * odd) % PLANES, i)
            answer(k, AT_UP, A + 8 + inner, BLOCK_A, down1, i)
            answer(k, AT_DOWN, B + 8 + inner, BLOCK_B, up1, i)
            return 0

        lax.fori_loop(0, GROUP, send_far, 0)
        lax.fori_loop(2, 4, part, 0)
        answer_plane(k, ways[0:2])

    def answer(k, at, group, block, to_z, i):
        remote(product.at[k, at * GROUP + i], returned.at[k, group], ret_send, ret_recv.at[block // 2, k], to_z, i, tp).start()

    def answer_plane(k, some):
        def send_own(j, _):
            to = (inner + j) % GROUP
            for at, block in some:
                answer(k, at, first_group[block] + inner, block, z, to)
            return 0

        lax.fori_loop(1, GROUP, send_own, 0)
        for at, block in some:
            returned[k, first_group[block] + inner] = product[k, at * GROUP + inner]

    def answer_near(k):
        answer_plane(k, ways[2:4])
        answer_plane(k, ways[4:5])

    def weighed(block, groups, k):
        rows = returned[k, pl.ds(first_group[block], groups)].reshape(groups * CAP, HALF)
        lanes = slice(LANE[block], LANE[block] + groups * CAP)
        return jnp.dot(high[:, lanes], rows, preferred_element_type=F32) + jnp.dot(
            low[:, lanes], rows, preferred_element_type=F32
        )

    def send_partials(k):
        landed(returned.at[k, pl.ds(0, 38)], ret_recv.at[0, k])
        far[0, k] = weighed(BLOCK_A, 20, k).astype(BF16)
        remote(far.at[0, k], far_in.at[0, k], far_send, far_recv.at[k], down1, inner, tp).start()
        far[1, k] = weighed(BLOCK_B, 20, k).astype(BF16)
        remote(far.at[1, k], far_in.at[1, k], far_send, far_recv.at[k], up1, inner, tp).start()

    def add_partials(k):
        landed(returned.at[k, pl.ds(0, 14)], ret_recv.at[1, k])
        landed(far_in.at[0, pl.ds(0, 2)], far_recv.at[k])
        for side, block, to in ((0, BLOCK_C, down1), (1, BLOCK_D, up1)):
            here = weighed(block, 8, k)
            near[side, k] = (here + far_in[side, k].astype(F32)).astype(BF16)
            remote(near.at[side, k], near_in.at[side, k], near_send, near_recv.at[k], to, inner, tp).start()

    def close(k):
        n, h = columns_at(k)
        landed(returned.at[k, pl.ds(0, 7)], ret_recv.at[2, k])
        here = weighed(BLOCK_E, 8, k)
        landed(near_in.at[0, pl.ds(0, 2)], near_recv.at[k])
        t = tokens[:, pl.ds(pl.multiple_of(n * COL + h * HALF, HALF), HALF)].astype(F32)
        r = (t + here + near_in[0, k].astype(F32) + near_in[1, k].astype(F32)).astype(BF16)
        residual[k] = r
        s = r.astype(F32)
        s = s * s
        s = s[:, 0:128] + s[:, 128:256]
        squares[...] = s if k == 0 else squares[...] + s

        @pl.when(n != tp)
        def _():
            remote(residual.at[k], slices.at[tp, h], slice_send, slice_recv.at[tp], z, inner, n).start()

        @pl.when(n == tp)
        def _():
            slices[tp, h] = residual[k]

    relay_down(1)
    contract(0)
    contract(1)
    answer_near(0)
    relay_down(2)
    answer_near(1)
    send_partials(0)
    contract(2)
    relay_down(3)
    send_partials(1)
    answer_near(2)
    contract(3)
    relay_down(4)
    answer_near(3)
    add_partials(0)
    send_partials(2)
    relay_down(5)
    add_partials(1)
    relay_down(6)
    close(0)
    contract(4)
    relay_down(7)
    answer_near(4)
    send_partials(3)
    add_partials(2)
    close(1)
    contract(5)
    answer_near(5)
    send_partials(4)
    add_partials(3)
    close(2)
    contract(6)
    answer_near(6)
    send_partials(5)
    add_partials(4)
    close(3)
    contract(7)
    answer_near(7)
    send_partials(6)
    add_partials(5)
    close(4)
    send_partials(7)
    add_partials(6)
    close(5)
    add_partials(7)
    close(6)
    close(7)

    inverse = lax.rsqrt(jnp.sum(squares[...], axis=-1, keepdims=True) / D + EPS)
    inverse_out[...] = jnp.broadcast_to(inverse, (ROWS, 128)).T[0:8, :]
    lasts = [
        remote(inverse_out, inverses.at[tp], inv_send, inv_recv.at[k], z, inner, other)
        for k, other in enumerate((right, left, opposite))
    ]
    start(lasts)
    inverses[tp] = inverse_out[...]

    def finish(source):
        column = jnp.broadcast_to(inverses[source, 0:1, :], (128, ROWS)).T[:, 0:1]
        for h in range(2):
            cols = slice(h * HALF, (h + 1) * HALF)
            t = slices[source, h].astype(F32) * column * final_gain[cols].astype(F32)[None, :]
            out[source, :, cols] = t.astype(BF16)

    finish(tp)
    for copy, other in zip(lasts, (left, right, opposite)):
        copy.wait_recv()
        landed(slices.at[other], slice_recv.at[other])
        finish(other)

    sent(info.at[pl.ds(0, 4)], info_send)
    sent(wgu.at[pl.ds(0, 3)], w_send)
    sent(wd.at[pl.ds(0, 3)], d_send)
    sent(inverses.at[pl.ds(0, 3)], inv_send)
    sent(raw, raw_send)
    sent(routed.at[pl.ds(0, 59)], disp_send)
    sent(routed.at[pl.ds(0, 59)], ret_send)
    sent(far, far_send)
    sent(near, near_send)
    sent(slices.at[pl.ds(0, 3)], slice_send)


def local(
    tokens, norm_gain, expert_ids, group_weight, expert_logit, w_gate, w_up, w_down, final_gain
):
    anywhere = pl.BlockSpec(memory_space=pl.ANY)
    dma, groups = pltpu.SemaphoreType.DMA, PLANES * GROUP
    out = pl.pallas_call(
        kernel,
        out_shape=pltpu.VMEM((TP, ROWS, COL), BF16),
        in_specs=[anywhere] * 9,
        out_specs=pl.BlockSpec(memory_space=pltpu.VMEM),
        scratch_shapes=[
            pltpu.VMEM((ROWS, D), BF16),
            pltpu.VMEM((D,), BF16),
            pltpu.VMEM((2, ROWS), jnp.int32),
            pltpu.VMEM((1, ROWS), F32),
            pltpu.VMEM((2, ROWS), F32),
            pltpu.VMEM((COL,), BF16),
            pltpu.VMEM((TP, ROWS, COL), BF16),
            pltpu.VMEM((4, TP, ROWS, COL), BF16),
            pltpu.VMEM((5, 8, ROWS), F32),
            pltpu.VMEM((groups * CAP, ROWS), BF16),
            pltpu.VMEM((groups, CAP, D), BF16),
            pltpu.VMEM((groups, CAP, D), BF16),
            pltpu.VMEM((TP, groups * CAP, FF // TP), BF16),
            pltpu.VMEM((STAGES, groups, CAP, HALF), BF16),
            pltpu.VMEM((STAGES, groups, CAP, HALF), BF16),
            pltpu.VMEM((TP, D, 2 * FF // TP), BF16),
            pltpu.VMEM((TP, TP, FF // TP, COL), BF16),
            pltpu.VMEM((ROWS, 1152), BF16),
            pltpu.VMEM((ROWS, 1152), BF16),
            pltpu.VMEM((2, STAGES, ROWS, HALF), BF16),
            pltpu.VMEM((2, STAGES, ROWS, HALF), BF16),
            pltpu.VMEM((2, STAGES, ROWS, HALF), BF16),
            pltpu.VMEM((2, STAGES, ROWS, HALF), BF16),
            pltpu.VMEM((STAGES, ROWS, HALF), BF16),
            pltpu.VMEM((TP, 2, ROWS, HALF), BF16),
            pltpu.VMEM((ROWS, 128), F32),
            pltpu.VMEM((8, ROWS), F32),
            pltpu.VMEM((TP, 8, ROWS), F32),
            dma((9,)), dma((6,)), dma, dma((6,)), dma, dma((STAGES, 2)), dma, dma((2,)), dma, dma((2, TP)),
            dma, dma((PLANES,)), dma, dma((3, STAGES)), dma, dma((STAGES,)), dma, dma((STAGES,)), dma, dma((TP,)),
            dma, dma((3,)),
        ],
        compiler_params=pltpu.CompilerParams(
            collective_id=0, has_side_effects=True, vmem_limit_bytes=62 * 1024 * 1024
        ),
    )(
        tokens, norm_gain, expert_ids.T, group_weight[None, :], expert_logit.T,
        w_gate[0], w_up[0], w_down[0], final_gain,
    )
    return out.reshape(TP * ROWS, COL)


def solution(mesh):
    placed = (
        P(("ep", "tp"), None),
        P(),
        P(("ep", "tp"), None),
        P(("ep", "tp")),
        P(("ep", "tp"), None),
        P("ep", None, "tp"),
        P("ep", None, "tp"),
        P("ep", "tp", None),
        P("tp"),
    )
    return jax.shard_map(
        local, mesh=mesh, in_specs=placed, out_specs=P("ep", "tp"), check_vma=False
    )
```
